256 devices in a mesh: grp: 2 (over y), kv: 16 (over z), tp: 8 (over x, core).
Axes of the slice: x: 4, y: 2, z: 16, core: 2. Of those that a mesh axis runs over, the one named last changes fastest.
The devices are a block of a 4x16x16 slice.
Arguments:
- residual: bfloat16 [32, 4096], P('grp', ('kv', 'tp')), parts along dimension 0, may hold values from -11 to 11
- cache_keys: bfloat16 [32, 16384, 8, 128], P('grp', 'kv', 'tp'), parts along dimension 0, may hold values from -210 to 210
- cache_values: bfloat16 [32, 16384, 8, 128], P('grp', 'kv', 'tp'), parts along dimension 0, may hold values from -6 to 6
- norm_gain: bfloat16 [4096], P('kv'), may hold values from 0.099609375 to 1.8984375
- query_weight: bfloat16 [4096, 2048], P('kv', 'tp'), may hold values from -0.09375 to 0.09375
- key_weight: bfloat16 [4096, 1024], P('kv', 'tp'), may hold values from -0.25 to 0.25
- value_weight: bfloat16 [4096, 1024], P('kv', 'tp'), may hold values from -0.375 to 0.375
- head_lambda: float32 [16], P('tp'), may hold values from 0.3 to 0.8
- head_gain: bfloat16 [128], replicated, may hold values from 0.099609375 to 1.8984375
- out_weight: bfloat16 [2048, 4096], P('tp', 'kv'), may hold values from -0.1875 to 0.1875
- mixer_gain: bfloat16 [4096], P('kv'), may hold values from 0.099609375 to 1.8984375
- up_weight: bfloat16 [4096, 16384], P('kv', 'tp'), may hold values from -0.09375 to 0.09375
- down_weight: bfloat16 [16384, 4096], P('tp', 'kv'), may hold values from -0.0625 to 0.0625
Outputs:
- updated: bfloat16 [32, 4096], P('grp', ('kv', 'tp')), parts along dimension 0
The draws below stay inside these ranges and needn't reach their ends.
There are 2 independent parts, one for each index of `grp`. The reference program is written for one: setup_inputs(seed, part) draws one part's arguments, and reference() takes and returns one part's arrays. A program takes and returns all parts, laid end to end along the dimension named above; an argument that names none is the same for every part. Nothing has to cross between parts.
All inputs are finite; a program needn't handle non-finite values.
Results may differ from the reference program's by a relative error of at most 0.018.
Values may be sent and summed in bfloat16 or wider, within the bound.
A program may use at most 64 MiB of HBM per device.

```python
import jax
import jax.numpy as jnp
from jax import lax

D = 4096
HEADS = 16
KV_HEADS = 8
HALF = 64
VDIM = 128
FF = 16384
BATCH = 16
CTX = 16384


def draw_residual(key, part):
    first, second = jax.random.split(key, 2)
    column = jnp.arange(D, dtype=jnp.float32)
    rough = jax.random.uniform(first, (D,), jnp.float32, 0.5, 1.5)
    scale = 0.15 * 8.0 ** (column / D) * rough
    base = jnp.clip(jax.random.normal(second, (BATCH, D), jnp.float32), -6.0, 6.0)
    return (base * scale).astype(jnp.bfloat16)


def draw_cache_keys(key, part):
    first = jax.random.fold_in(key, 0)
    base = 1.75 * jnp.clip(jax.random.normal(first, (BATCH, CTX, KV_HEADS, 2 * HALF), jnp.float32), -6.0, 6.0)
    return base.astype(jnp.bfloat16)


def raised(result, key, source, target, blocks, factor):
    owner, partner = [(jnp.arange(result.shape[dim]) // (result.shape[dim] // blocks)).reshape([-1 if axis == dim else 1 for axis in range(result.ndim)]) for dim in (source, target)]
    chosen = jax.random.permutation(key, blocks)[partner]
    strong = (owner == chosen) | (owner == (partner + blocks // 2) % blocks)
    return jnp.where(strong, factor * result, result)


def levels(key, extent, shards, smallest, largest):
    def one(dim, blocks):
        draws = jax.random.uniform(jax.random.fold_in(jax.random.fold_in(key, 6), dim), (blocks,), jnp.float32, smallest / len(shards), largest / len(shards))
        return jnp.repeat(jnp.exp(draws), extent[dim] // blocks).reshape((-1,) + (1,) * (len(extent) - dim - 1))

    loudness = one(*shards[0])
    for cut in shards[1:]:
        loudness = loudness * one(*cut)
    return loudness


def normal_values(key, extent, deviation, most, shards=(), held_as=jnp.bfloat16):
    drawn = jax.random.normal(key, extent, jnp.float32) * deviation
    if len(shards) > 0:
        drawn = levels(key, extent, shards, -0.22, 0.18) * drawn
    return jnp.clip(drawn, min=-most, max=most).astype(held_as)


def bell_draw_with(own_key, dims, scale, most, cuts, heavy, kind=jnp.bfloat16):
    values = scale * jax.random.normal(own_key, dims, jnp.float32)
    if cuts:
        values = values * levels(own_key, dims, cuts, -0.22, 0.18)
    return jnp.clip(raised(values, jax.random.fold_in(own_key, 3), *heavy), -most, most).astype(kind)


def setup_inputs(seed: int = 0, part: int = 0) -> dict:
    streams_of = jax.random.split(jax.random.key(seed), 14)
    own_keys = jax.random.split(jax.random.fold_in(streams_of[13], part), 14)
    return {
        "residual": draw_residual(jax.random.fold_in(jax.random.fold_in(streams_of[13], part), 71), part),
        "cache_keys": draw_cache_keys(jax.random.fold_in(jax.random.fold_in(streams_of[13], part), 71), part),
        "cache_values": normal_values(own_keys[2], (BATCH, CTX, KV_HEADS, VDIM), 1.0, 6.0, ((1, 16), (2, 8))),
        "norm_gain": jnp.clip(1.0 + 0.18 * jax.random.normal(streams_of[3], (D,), jnp.float32), 0.099609375, 1.8984375).astype(jnp.bfloat16),
        "query_weight": normal_values(streams_of[4], (D, HEADS * 2 * HALF), D ** -0.5, 0.09375, ((0, 16), (1, 8))),
        "key_weight": normal_values(streams_of[5], (D, KV_HEADS * 2 * HALF), (D // 9) ** -0.5, 0.25, ((0, 16), (1, 8))),
        "value_weight": normal_values(streams_of[6], (D, KV_HEADS * VDIM), (D // 16) ** -0.5, 0.375, ((0, 16), (1, 8))),
        "head_lambda": jnp.clip(0.3 + 0.5 * jax.random.uniform(streams_of[7], (HEADS,), jnp.float32) ** levels(streams_of[7], (HEADS,), ((0, 8),), -0.2, 0.2), 0.3, 0.8),
        "head_gain": jnp.clip(1.0 + 0.18 * jax.random.normal(streams_of[8], (VDIM,), jnp.float32), 0.099609375, 1.8984375).astype(jnp.bfloat16),
        "out_weight": bell_draw_with(streams_of[9], (HEADS * VDIM, D), (HEADS * VDIM) ** -0.5, 0.1875, ((0, 8), (1, 16)), (0, 1, 16, 2.0)),
        "mixer_gain": jnp.clip(1.0 + 0.18 * jax.random.normal(streams_of[10], (D,), jnp.float32), 0.099609375, 1.8984375).astype(jnp.bfloat16),
        "up_weight": normal_values(streams_of[11], (D, FF), D ** -0.5, 0.09375, ((0, 16), (1, 8))),
        "down_weight": bell_draw_with(streams_of[12], (FF, D), FF ** -0.5, 0.0625, ((0, 8), (1, 16)), (0, 1, 16, 2.0)),
    }


EPS = 1e-06

def reference(residual, cache_keys, cache_values, norm_gain, query_weight, key_weight, value_weight, head_lambda, head_gain, out_weight, mixer_gain, up_weight, down_weight):
    f32 = jnp.float32
    bf16 = jnp.bfloat16
    group = HEADS // KV_HEADS
    scale = 1.0 / HALF ** 0.5
    resid = residual.astype(f32)
    scaled = (resid * norm_gain.astype(f32)).astype(bf16)
    inv_rms = lax.rsqrt(lax.optimization_barrier(jnp.mean(resid * resid, axis=1, keepdims=True)) + EPS)
    query = (inv_rms * jnp.dot(scaled, query_weight, preferred_element_type=f32)).astype(bf16)
    new_key = (inv_rms * jnp.dot(scaled, key_weight, preferred_element_type=f32)).astype(bf16)
    new_value = (inv_rms * jnp.dot(scaled, value_weight, preferred_element_type=f32)).astype(bf16)
    query = jnp.moveaxis(query.reshape(BATCH, KV_HEADS, group, 2, HALF), 1, 0)
    new_key = jnp.moveaxis(new_key.reshape(BATCH, KV_HEADS, 2, HALF), 1, 0)
    new_value = jnp.moveaxis(new_value.reshape(BATCH, KV_HEADS, VDIM), 1, 0)

    def one_head(args):
        q_head, k_own, v_own, index = args
        keys = lax.dynamic_index_in_dim(cache_keys, index, 2, keepdims=False).reshape(BATCH, CTX, 2, HALF)
        values = lax.dynamic_index_in_dim(cache_values, index, 2, keepdims=False)
        scores = jnp.einsum('bgch,bpch->bgcp', q_head.astype(f32), keys.astype(f32)) * scale
        cache_top = lax.optimization_barrier(jnp.max(scores, axis=3))
        expo = jnp.exp(scores - cache_top[..., None])
        total = lax.optimization_barrier(jnp.sum(expo, axis=3))
        probs = expo.astype(bf16)
        weighted = jnp.einsum('bgcp,bpv->bgcv', probs.astype(f32), values.astype(f32))
        own = jnp.einsum('bgch,bch->bgc', q_head.astype(f32), k_own.astype(f32)) * scale
        top = jnp.maximum(cache_top, own)
        old_part = jnp.exp(cache_top - top)
        own_part = jnp.exp(own - top)
        numer = weighted * old_part[..., None] + own_part[..., None] * v_own.astype(f32)[:, None, None, :]
        return numer / (total * old_part + own_part)[..., None]
    attended = lax.map(one_head, (query, new_key, new_value, jnp.arange(KV_HEADS, dtype=jnp.int32)))
    attended = jnp.moveaxis(attended, 0, 1).reshape(BATCH, HEADS, 2, VDIM)
    diff = attended[:, :, 0] - head_lambda[None, :, None] * attended[:, :, 1]
    normed = diff * lax.rsqrt(lax.optimization_barrier(jnp.mean(diff * diff, axis=2, keepdims=True)) + EPS) * head_gain.astype(f32)
    heads_out = normed.astype(bf16).reshape(BATCH, HEADS * VDIM)
    mixed = (resid + jnp.dot(heads_out, out_weight, preferred_element_type=f32)).astype(bf16)
    mixed_f = mixed.astype(f32)
    scaled2 = (mixed_f * mixer_gain.astype(f32)).astype(bf16)
    inv_rms2 = lax.rsqrt(lax.optimization_barrier(jnp.mean(mixed_f * mixed_f, axis=1, keepdims=True)) + EPS)
    up = inv_rms2 * jnp.dot(scaled2, up_weight, preferred_element_type=f32)
    hidden = jnp.square(jnp.maximum(up, 0.0)).astype(bf16)
    return (mixed_f + jnp.dot(hidden, down_weight, preferred_element_type=f32)).astype(bf16)
```

```python
import functools

import jax
import jax.numpy as jnp
from jax import lax
from jax.experimental import pallas as pl
from jax.experimental.pallas import tpu as pltpu
from jax.sharding import PartitionSpec as P

EPS = 1e-06
MESH = pl.DeviceIdType.MESH
F32 = jnp.float32
BF16 = jnp.bfloat16
LANES = 128
LOW = -1e30


def far_first(n):
    order = [n // 2]
    for k in range(1, n // 2 + 1):
        for d in (n // 2 - k, n // 2 + k):
            if 0 < d < n:
                order.append(d)
    return order


def iota(shape, dim):
    return lax.broadcasted_iota(jnp.int32, shape, dim)


def dot(a, b):
    return jnp.dot(a, b, preferred_element_type=F32)


def to_lanes(column):
    wide = jnp.broadcast_to(column, (column.shape[0], LANES))
    diagonal = iota(wide.shape, 0) == iota(wide.shape, 1)
    return jnp.sum(jnp.where(diagonal, wide, 0.0), axis=0, keepdims=True)


def to_rows(row, rows):
    wide = jnp.broadcast_to(row, (rows, LANES))
    diagonal = iota(wide.shape, 0) == iota(wide.shape, 1)
    return jnp.sum(jnp.where(diagonal, wide, 0.0), axis=1, keepdims=True)


def kernel(
    KV,
    TP,
    res_h,
    keys_h,
    values_h,
    ng_h,
    wq_h,
    wk_h,
    wv_h,
    lam_h,
    hg_h,
    wo_h,
    mg_h,
    wu_h,
    wd_h,
    out_ref,
    res,
    keys,
    values,
    ng,
    wp,
    lam,
    hg,
    wo,
    mg,
    wu,
    wd,
    abuf,
    qbuf,
    kvs,
    kvr,
    wbuf,
    mlbuf,
    dbuf,
    sqbuf,
    us,
    ur,
    hbuf,
    fs,
    fr,
    load_sem,
    a_send,
    a_recv,
    q_send,
    q_recv,
    r_send,
    r_recv,
    w_send,
    w_recv,
    m_send,
    m_recv,
    d_send,
    d_recv,
    s_send,
    s_recv,
    u_send,
    u_recv,
    h_send,
    h_recv,
    f_send,
    f_recv,
):
    z = lax.axis_index("kv")
    t = lax.axis_index("tp")
    rows = res_h.shape[0]
    piece = res_h.shape[1]
    per_tile = LANES // piece
    width = wo.shape[1]
    D = KV * width
    qcols = wq_h.shape[1]
    heads = qcols // LANES
    half = LANES // 2
    maps = heads * 2
    lines = rows * maps

    def load(src, dst, k):
        copy = pltpu.make_async_copy(src, dst, load_sem.at[k])
        copy.start()
        return copy

    ld_res = load(res_h, res, 0)
    for u in range(1, TP):
        peer = lax.rem(t + u, TP)
        pl.semaphore_signal(
            pltpu.get_barrier_semaphore(), inc=1, device_id={"tp": peer}, device_id_type=MESH
        )
    for u in far_first(KV):
        peer = lax.rem(z + u, KV)
        pl.semaphore_signal(
            pltpu.get_barrier_semaphore(), inc=1, device_id={"kv": peer}, device_id_type=MESH
        )
    ld_ng = load(ng_h, ng, 1)
    ld_wq = load(wq_h, wp.at[:, 0:qcols], 2)
    ld_wk = load(wk_h, wp.at[:, qcols : qcols + LANES], 3)
    ld_wv = load(wv_h, wp.at[:, qcols + LANES : qcols + 2 * LANES], 4)
    ld_keys = load(keys_h, keys, 5)
    ld_values = load(values_h, values, 6)
    ld_lam = load(lam_h, lam, 7)
    ld_hg = load(hg_h, hg, 8)
    ld_wo = load(wo_h, wo, 9)
    ld_mg = load(mg_h, mg, 10)
    ld_wu = load(wu_h, wu, 11)
    ld_wd = load(wd_h, wd, 12)

    started = []

    def send(src, dst, ssem, rsem, axis, peer):
        copy = pltpu.make_async_remote_copy(
            src_ref=src,
            dst_ref=dst,
            send_sem=ssem,
            recv_sem=rsem,
            device_id={axis: peer},
            device_id_type=MESH,
        )
        copy.start()
        started.append(copy)
        return copy

    kv_order = far_first(KV)
    tp_order = far_first(TP)

    def spread(src_of, dst, sems, rsems, axis):
        me, n, order = (z, KV, kv_order) if axis == "kv" else (t, TP, tp_order)
        copies = []
        for d in order:
            peer = lax.rem(me + d, n)
            copies.append(send(src_of(peer), dst.at[me], sems.at[d - 1], rsems.at[d - 1], axis, peer))
        return copies

    def arrive(copies):
        for copy in copies:
            copy.wait_recv()

    ld_res.wait()
    own_piece = res[...].astype(F32)
    tiled = jnp.concatenate([own_piece] * per_tile, axis=1)
    at = iota(tiled.shape, 1) // piece == lax.rem(t, per_tile)
    abuf[t] = jnp.where(at, tiled, 0.0).astype(BF16)
    pl.semaphore_wait(pltpu.get_barrier_semaphore(), TP - 1 + KV - 1)
    arrive(spread(lambda peer: abuf.at[t], abuf, a_send, a_recv, "tp"))
    block = jnp.concatenate(
        [
            sum(abuf[k * per_tile + j].astype(F32) for j in range(per_tile))
            for k in range(TP // per_tile)
        ],
        axis=1,
    )
    ld_ng.wait()
    gain = jnp.concatenate([ng[k : k + 1, :] for k in range(width // LANES)], axis=1).astype(F32)
    scaled = (block * gain).astype(BF16)
    ld_wq.wait()
    ld_wk.wait()
    ld_wv.wait()
    proj = dot(scaled, wp[...])
    qbuf[z] = proj[:, 0:qcols].astype(BF16)
    square = to_lanes(jnp.sum(block * block, axis=1, keepdims=True))
    for j in range(KV):
        kvs[j] = jnp.concatenate([proj[j : j + 1, qcols:], square], axis=1)
    kvr[z] = kvs[z]
    q_copies = spread(lambda peer: qbuf.at[z], qbuf, q_send, q_recv, "kv")
    r_copies = spread(lambda peer: kvs.at[peer], kvr, r_send, r_recv, "kv")
    arrive(q_copies)
    arrive(r_copies)
    q_sum = qbuf[0].astype(F32)
    r_sum = kvr[0]
    for j in range(1, KV):
        q_sum = q_sum + qbuf[j].astype(F32)
        r_sum = r_sum + kvr[j]
    inv_lanes = lax.rsqrt(r_sum[:, 2 * LANES :] / D + EPS)
    inv_own = jnp.sum(
        jnp.where(iota(inv_lanes.shape, 1) == z, inv_lanes, 0.0), axis=1, keepdims=True
    )
    new_key = (inv_own * r_sum[:, 0:LANES]).astype(BF16).astype(F32)
    new_value = (inv_own * r_sum[:, LANES : 2 * LANES]).astype(BF16).astype(F32)
    query = (to_rows(inv_lanes, rows) * q_sum).astype(BF16)

    pick = (iota((lines, rows), 0) // maps == iota((lines, rows), 1)).astype(BF16)
    spreadq = dot(pick, query)
    line = iota((lines, LANES), 0)
    chosen = spreadq[:, 0:LANES]
    for g in range(1, heads):
        chosen = jnp.where(
            lax.rem(line, maps) // 2 == g, spreadq[:, g * LANES : (g + 1) * LANES], chosen
        )
    mine = iota((lines, LANES), 1) // half == lax.rem(line, 2)
    lined = jnp.where(mine, chosen, 0.0) * (1.0 / half**0.5)

    ld_keys.wait()
    ld_values.wait()
    tops, totals, sums = [], [], []
    for p in range(lines // 8):
        seqs = 8 // maps
        qp = lined[8 * p : 8 * p + 8, :].astype(BF16)
        scores = None
        for k in range(seqs):
            part = lax.dot_general(
                qp, keys[seqs * p + k], (((1,), (1,)), ((), ())), preferred_element_type=F32
            )
            if scores is None:
                scores = part
            else:
                scores = jnp.where(iota(part.shape, 0) // maps == k, part, scores)
        top = jnp.max(scores, axis=1, keepdims=True)
        expo = jnp.exp(scores - top)
        total = jnp.sum(expo, axis=1, keepdims=True)
        probs = expo.astype(BF16)
        weighted = None
        for k in range(seqs):
            part = dot(probs, values[seqs * p + k])
            if weighted is None:
                weighted = part
            else:
                weighted = jnp.where(iota(part.shape, 0) // maps == k, part, weighted)
        tops.append(top)
        totals.append(total)
        sums.append(weighted)
    top = jnp.concatenate(tops, axis=0)
    total = jnp.concatenate(totals, axis=0)
    weighted = jnp.concatenate(sums, axis=0)
    own = jnp.sum(lined * new_key, axis=1, keepdims=True)
    own = jnp.where(iota(own.shape, 0) // maps == z, own, LOW)
    new_top = jnp.maximum(top, own)
    old_part = jnp.exp(top - new_top)
    own_part = jnp.exp(own - new_top)
    total = total * old_part + own_part
    weighted = weighted * old_part + own_part * new_value
    wbuf[z] = weighted.astype(BF16)
    lane = iota((lines, LANES), 1)
    both = jnp.where(lane == line, new_top, jnp.where(lane == line + half, total, 0.0))
    mlbuf[z] = jnp.sum(both, axis=0, keepdims=True)
    m_copies = spread(lambda peer: mlbuf.at[z], mlbuf, m_send, m_recv, "kv")
    w_copies = spread(lambda peer: wbuf.at[z], wbuf, w_send, w_recv, "kv")
    arrive(m_copies)
    ml = jnp.concatenate([mlbuf[j] for j in range(KV)], axis=0)
    shares = jnp.exp(ml - jnp.max(ml, axis=0, keepdims=True))
    grand = jnp.sum(shares * pltpu.roll(ml, half, 1), axis=0, keepdims=True)
    in_use = iota(ml.shape, 1) < half
    shares = jnp.where(in_use, shares / jnp.where(in_use[0:1], grand, 1.0), 0.0)
    columns = jnp.transpose(shares)
    arrive(w_copies)
    attended = columns[0:lines, 0:1] * wbuf[0].astype(F32)
    for j in range(1, KV):
        attended = attended + columns[0:lines, j : j + 1] * wbuf[j].astype(F32)
    ld_lam.wait()
    ld_hg.wait()
    lambdas = lam[0:1, 0:1]
    for g in range(1, heads):
        lambdas = jnp.where(
            lax.rem(iota((lines, 1), 0), maps) // 2 == g, lam[0:1, g : g + 1], lambdas
        )
    diff = attended - lambdas * pltpu.roll(attended, lines - 1, 0)
    normed = (
        diff
        * lax.rsqrt(jnp.mean(diff * diff, axis=1, keepdims=True) + EPS)
        * hg[...].astype(F32)
    ).astype(BF16)
    outs = []
    for g in range(heads):
        pick = iota((rows, lines), 1) == iota((rows, lines), 0) * maps + 2 * g
        outs.append(dot(pick.astype(BF16), normed))
    heads_out = jnp.concatenate(outs, axis=1).astype(BF16)
    ld_wo.wait()
    dbuf[t] = dot(heads_out, wo[...])
    arrive(spread(lambda peer: dbuf.at[t], dbuf, d_send, d_recv, "tp"))
    projected = dbuf[0]
    for j in range(1, TP):
        projected = projected + dbuf[j]
    mixed = (block + projected).astype(BF16).astype(F32)
    sqbuf[z] = to_lanes(jnp.sum(mixed * mixed, axis=1, keepdims=True))
    s_copies = spread(lambda peer: sqbuf.at[z], sqbuf, s_send, s_recv, "kv")
    ld_mg.wait()
    gain2 = jnp.concatenate([mg[k : k + 1, :] for k in range(width // LANES)], axis=1).astype(F32)
    scaled2 = (mixed * gain2).astype(BF16)
    ld_wu.wait()
    up = dot(scaled2, wu[...])
    share_width = up.shape[1] // KV
    for j in range(KV):
        us[j] = up[:, j * share_width : (j + 1) * share_width].astype(us.dtype)
    ur[z] = us[z]
    u_copies = spread(lambda peer: us.at[peer], ur, u_send, u_recv, "kv")
    arrive(s_copies)
    square2 = sqbuf[0]
    for j in range(1, KV):
        square2 = square2 + sqbuf[j]
    inv2 = to_rows(lax.rsqrt(square2 / D + EPS), rows)
    arrive(u_copies)
    up_sum = ur[0].astype(F32)
    for j in range(1, KV):
        up_sum = up_sum + ur[j].astype(F32)
    act = jnp.maximum(inv2 * up_sum, 0.0)
    hbuf[z] = (act * act).astype(BF16)
    arrive(spread(lambda peer: hbuf.at[z], hbuf, h_send, h_recv, "kv"))
    hidden = jnp.concatenate([hbuf[j] for j in range(KV)], axis=1)
    ld_wd.wait()
    down = dot(hidden, wd[...])
    for k in range(width // LANES):
        fs[k] = down[:, k * LANES : (k + 1) * LANES]
    fr[t] = fs[t // per_tile]
    arrive(spread(lambda peer: fs.at[peer // per_tile], fr, f_send, f_recv, "tp"))
    y = fr[0]
    for j in range(1, TP):
        y = y + fr[j]
    for k in range(width // LANES):
        y = y + jnp.where(t // per_tile == k, mixed[:, k * LANES : (k + 1) * LANES], 0.0)
    result = y[:, 0:piece]
    for k in range(1, per_tile):
        result = jnp.where(lax.rem(t, per_tile) == k, y[:, k * piece : (k + 1) * piece], result)
    out_ref[...] = result.astype(out_ref.dtype)
    for copy in started:
        copy.wait_send()


def body(
    KV,
    TP,
    residual,
    cache_keys,
    cache_values,
    norm_gain,
    query_weight,
    key_weight,
    value_weight,
    head_lambda,
    head_gain,
    out_weight,
    mixer_gain,
    up_weight,
    down_weight,
):
    rows, piece = residual.shape
    positions, depth = cache_keys.shape[1], cache_keys.shape[3]
    width = out_weight.shape[1]
    qcols = query_weight.shape[1]
    lines = rows * qcols * 2 // LANES
    share = up_weight.shape[1] // KV
    any_spec = pl.BlockSpec(memory_space=pl.ANY)
    dma = pltpu.SemaphoreType.DMA
    keys = cache_keys.reshape(rows, positions, depth)
    values = cache_values.reshape(rows, positions, depth)
    args = (
        residual,
        keys,
        values,
        norm_gain.reshape(width // LANES, LANES),
        query_weight,
        key_weight,
        value_weight,
        head_lambda.reshape(1, -1),
        head_gain.reshape(1, -1),
        out_weight,
        mixer_gain.reshape(width // LANES, LANES),
        up_weight,
        down_weight,
    )
    kv_sems = [dma((KV - 1,))] * 2
    tp_sems = [dma((TP - 1,))] * 2
    return pl.pallas_call(
        functools.partial(kernel, KV, TP),
        out_shape=jax.ShapeDtypeStruct((rows, piece), residual.dtype),
        in_specs=[any_spec] * len(args),
        out_specs=pl.BlockSpec(memory_space=pltpu.VMEM),
        scratch_shapes=[
            pltpu.VMEM((rows, piece), BF16),
            pltpu.VMEM(keys.shape, BF16),
            pltpu.VMEM(values.shape, BF16),
            pltpu.VMEM((width // LANES, LANES), BF16),
            pltpu.VMEM((width, qcols + 2 * LANES), BF16),
            pltpu.VMEM((1, head_lambda.shape[0]), F32),
            pltpu.VMEM((1, head_gain.shape[0]), BF16),
            pltpu.VMEM(out_weight.shape, BF16),
            pltpu.VMEM((width // LANES, LANES), BF16),
            pltpu.VMEM(up_weight.shape, BF16),
            pltpu.VMEM(down_weight.shape, BF16),
            pltpu.VMEM((TP, rows, LANES), BF16),
            pltpu.VMEM((KV, rows, qcols), BF16),
            pltpu.VMEM((KV, 1, 3 * LANES), F32),
            pltpu.VMEM((KV, 1, 3 * LANES), F32),
            pltpu.VMEM((KV, lines, LANES), BF16),
            pltpu.VMEM((KV, 1, LANES), F32),
            pltpu.VMEM((TP, rows, width), F32),
            pltpu.VMEM((KV, 1, LANES), F32),
            pltpu.VMEM((KV, rows, share), F32),
            pltpu.VMEM((KV, rows, share), F32),
            pltpu.VMEM((KV, rows, share), BF16),
            pltpu.VMEM((width // LANES, rows, LANES), F32),
            pltpu.VMEM((TP, rows, LANES), F32),
            dma((13,)),
            *tp_sems,
            *kv_sems,
            *kv_sems,
            *kv_sems,
            *kv_sems,
            *tp_sems,
            *kv_sems,
            *kv_sems,
            *kv_sems,
            *tp_sems,
        ],
        compiler_params=pltpu.CompilerParams(
            collective_id=0, has_side_effects=True, vmem_limit_bytes=48 * 1024 * 1024
        ),
        name="layer",
    )(*args)


def solution(mesh):
    in_specs = (
        P("grp", ("kv", "tp")),
        P("grp", "kv", "tp", None),
        P("grp", "kv", "tp", None),
        P("kv"),
        P("kv", "tp"),
        P("kv", "tp"),
        P("kv", "tp"),
        P("tp"),
        P(),
        P("tp", "kv"),
        P("kv"),
        P("kv", "tp"),
        P("tp", "kv"),
    )
    out_specs = P("grp", ("kv", "tp"))
    fn = functools.partial(body, mesh.shape["kv"], mesh.shape["tp"])
    return jax.shard_map(fn, mesh=mesh, in_specs=in_specs, out_specs=out_specs, check_vma=False)
```

```python
import functools

import jax
import jax.numpy as jnp
from jax import lax
from jax.experimental import pallas as pl
from jax.experimental.pallas import tpu as pltpu
from jax.sharding import PartitionSpec as P

EPS = 1e-06
MESH = pl.DeviceIdType.MESH
F32 = jnp.float32
BF16 = jnp.bfloat16
LANES = 128
LOW = -1e30


def far_first(n):
    order = [n // 2]
    for k in range(1, n // 2 + 1):
        for d in (n // 2 - k, n // 2 + k):
            if 0 < d < n:
                order.append(d)
    return order


def iota(shape, dim):
    return lax.broadcasted_iota(jnp.int32, shape, dim)


def dot(a, b):
    return jnp.dot(a, b, preferred_element_type=F32)


def to_lanes(column):
    wide = jnp.broadcast_to(column, (column.shape[0], LANES))
    diagonal = iota(wide.shape, 0) == iota(wide.shape, 1)
    return jnp.sum(jnp.where(diagonal, wide, 0.0), axis=0, keepdims=True)


def to_rows(row, rows):
    wide = jnp.broadcast_to(row, (rows, LANES))
    diagonal = iota(wide.shape, 0) == iota(wide.shape, 1)
    return jnp.sum(jnp.where(diagonal, wide, 0.0), axis=1, keepdims=True)


def kernel(
    KV,
    TP,
    res_h,
    keys_h,
    values_h,
    ng_h,
    wq_h,
    wk_h,
    wv_h,
    lam_h,
    hg_h,
    wo_h,
    mg_h,
    wu_h,
    wd_h,
    out_ref,
    res,
    keys,
    values,
    ng,
    wp,
    lam,
    hg,
    wo,
    mg,
    wu,
    wd,
    abuf,
    qbuf,
    kvs,
    kvr,
    wsend,
    wbuf,
    mlsend,
    mlbuf,
    nbuf,
    dbuf,
    sqbuf,
    us,
    ur,
    hbuf,
    fs,
    fr,
    ring_sem,
    load_sem,
    a_send,
    a_recv,
    q_send,
    q_recv,
    r_send,
    r_recv,
    w_send,
    w_recv,
    m_send,
    m_recv,
    n_send,
    n_recv,
    d_send,
    d_recv,
    s_send,
    s_recv,
    u_send,
    u_recv,
    h_send,
    h_recv,
    f_send,
    f_recv,
):
    z = lax.axis_index("kv")
    t = lax.axis_index("tp")
    rows = res_h.shape[0]
    piece = res_h.shape[1]
    per_tile = LANES // piece
    width = wo.shape[1]
    D = KV * width
    qcols = wq_h.shape[1]
    heads = qcols // LANES
    half = LANES // 2
    maps = heads * 2
    lines = rows * maps

    def load(src, dst, k):
        copy = pltpu.make_async_copy(src, dst, load_sem.at[k])
        copy.start()
        return copy

    ld_res = load(res_h, res, 0)
    barrier = pltpu.get_barrier_semaphore()
    for u in range(1, TP):
        peer = lax.rem(t + u, TP)
        pl.semaphore_signal(barrier, inc=1, device_id={"tp": peer}, device_id_type=MESH)

    def both_ways(sem, d):
        for u in (d, KV - d):
            peer = lax.rem(z + u, KV)
            pl.semaphore_signal(sem, inc=1, device_id={"kv": peer}, device_id_type=MESH)

    both_ways(barrier, 1)
    ld_ng = load(ng_h, ng, 1)
    ld_wq = load(wq_h, wp.at[:, 0:qcols], 2)
    ld_wk = load(wk_h, wp.at[:, qcols : qcols + LANES], 3)
    ld_wv = load(wv_h, wp.at[:, qcols + LANES : qcols + 2 * LANES], 4)
    ld_keys = load(keys_h, keys, 5)
    ld_values = load(values_h, values, 6)
    ld_lam = load(lam_h, lam, 7)
    ld_hg = load(hg_h, hg, 8)
    ld_wo = load(wo_h, wo, 9)
    ld_mg = load(mg_h, mg, 10)
    ld_wu = load(wu_h, wu, 11)
    ld_wd = load(wd_h, wd, 12)

    started = []

    def send(src, dst, ssem, rsem, axis, peer):
        copy = pltpu.make_async_remote_copy(
            src_ref=src,
            dst_ref=dst,
            send_sem=ssem,
            recv_sem=rsem,
            device_id={axis: peer},
            device_id_type=MESH,
        )
        copy.start()
        started.append(copy)
        return copy

    kv_order = far_first(KV)
    tp_order = far_first(TP)

    def spread(src_of, dst, sems, rsems, axis, order=None):
        me, n = (z, KV) if axis == "kv" else (t, TP)
        if order is None:
            order = kv_order if axis == "kv" else tp_order
        copies = []
        for d in order:
            peer = lax.rem(me + d, n)
            copies.append(send(src_of(peer), dst, sems.at[d - 1], rsems.at[d - 1], axis, peer))
        return copies

    def arrive(copies):
        for copy in copies:
            copy.wait_recv()

    ld_res.wait()
    own_piece = res[...].astype(F32)
    tiled = jnp.concatenate([own_piece] * per_tile, axis=1)
    at = iota(tiled.shape, 1) // piece == lax.rem(t, per_tile)
    abuf[t] = jnp.where(at, tiled, 0.0).astype(BF16)
    pl.semaphore_wait(barrier, TP - 1 + 2)
    a_copies = spread(lambda peer: abuf.at[t], abuf.at[t], a_send, a_recv, "tp")
    both_ways(ring_sem.at[0], 1)
    pl.semaphore_wait(ring_sem.at[0], 2)
    both_ways(ring_sem.at[1], 2)
    arrive(a_copies)
    pl.semaphore_wait(ring_sem.at[1], 2)
    both_ways(ring_sem.at[2], 4)
    block = jnp.concatenate(
        [
            sum(abuf[k * per_tile + j].astype(F32) for j in range(per_tile))
            for k in range(TP // per_tile)
        ],
        axis=1,
    )
    ld_ng.wait()
    gain = jnp.concatenate([ng[k : k + 1, :] for k in range(width // LANES)], axis=1).astype(F32)
    scaled = (block * gain).astype(BF16)
    ld_wq.wait()
    ld_wk.wait()
    ld_wv.wait()
    proj = dot(scaled, wp[...])
    qbuf[z] = proj[:, 0:qcols].astype(BF16)
    square = to_lanes(jnp.sum(block * block, axis=1, keepdims=True))
    for j in range(KV):
        kvs[j] = jnp.concatenate([proj[j : j + 1, qcols:], square], axis=1)
    kvr[z] = kvs[z]
    pl.semaphore_wait(ring_sem.at[2], 2)
    q_copies = spread(lambda peer: qbuf.at[z], qbuf.at[z], q_send, q_recv, "kv")
    r_copies = spread(lambda peer: kvs.at[peer], kvr.at[z], r_send, r_recv, "kv")
    arrive(q_copies)
    arrive(r_copies)
    q_sum = qbuf[0].astype(F32)
    r_sum = kvr[0]
    for j in range(1, KV):
        q_sum = q_sum + qbuf[j].astype(F32)
        r_sum = r_sum + kvr[j]
    inv_lanes = lax.rsqrt(r_sum[:, 2 * LANES :] / D + EPS)
    inv_own = jnp.sum(
        jnp.where(iota(inv_lanes.shape, 1) == z, inv_lanes, 0.0), axis=1, keepdims=True
    )
    new_key = (inv_own * r_sum[:, 0:LANES]).astype(BF16).astype(F32)
    new_value = (inv_own * r_sum[:, LANES : 2 * LANES]).astype(BF16).astype(F32)
    query = (to_rows(inv_lanes, rows) * q_sum).astype(BF16)

    pick = (iota((lines, rows), 0) // maps == iota((lines, rows), 1)).astype(BF16)
    spreadq = dot(pick, query)
    line = iota((lines, LANES), 0)
    chosen = spreadq[:, 0:LANES]
    for g in range(1, heads):
        chosen = jnp.where(
            lax.rem(line, maps) // 2 == g, spreadq[:, g * LANES : (g + 1) * LANES], chosen
        )
    mine = iota((lines, LANES), 1) // half == lax.rem(line, 2)
    lined = jnp.where(mine, chosen, 0.0) * (1.0 / half**0.5)

    ld_keys.wait()
    ld_values.wait()
    tops, totals, sums = [], [], []
    for p in range(lines // 8):
        seqs = 8 // maps
        qp = lined[8 * p : 8 * p + 8, :].astype(BF16)
        scores = None
        for k in range(seqs):
            part = lax.dot_general(
                qp, keys[seqs * p + k], (((1,), (1,)), ((), ())), preferred_element_type=F32
            )
            if scores is None:
                scores = part
            else:
                scores = jnp.where(iota(part.shape, 0) // maps == k, part, scores)
        top = jnp.max(scores, axis=1, keepdims=True)
        expo = jnp.exp(scores - top)
        total = jnp.sum(expo, axis=1, keepdims=True)
        probs = expo.astype(BF16)
        weighted = None
        for k in range(seqs):
            part = dot(probs, values[seqs * p + k])
            if weighted is None:
                weighted = part
            else:
                weighted = jnp.where(iota(part.shape, 0) // maps == k, part, weighted)
        tops.append(top)
        totals.append(total)
        sums.append(weighted)
    top = jnp.concatenate(tops, axis=0)
    total = jnp.concatenate(totals, axis=0)
    weighted = jnp.concatenate(sums, axis=0)
    own = jnp.sum(lined * new_key, axis=1, keepdims=True)
    own = jnp.where(iota(own.shape, 0) // maps == z, own, LOW)
    new_top = jnp.maximum(top, own)
    old_part = jnp.exp(top - new_top)
    own_part = jnp.exp(own - new_top)
    total = total * old_part + own_part
    weighted = weighted * old_part + own_part * new_value
    quarter = lines // 4
    mine = lax.rem(z, 4)
    lane = iota((quarter, LANES), 1)
    line = iota((quarter, LANES), 0)
    for c in range(4):
        at = slice(c * quarter, (c + 1) * quarter)
        wsend[c] = weighted[at].astype(BF16)
        both = jnp.where(lane == line, new_top[at], jnp.where(lane == line + half, total[at], 0.0))
        mlsend[c] = jnp.sum(both, axis=0, keepdims=True)
    wbuf[z] = wsend[mine]
    mlbuf[z] = mlsend[mine]
    m_copies = spread(lambda peer: mlsend.at[lax.rem(peer, 4)], mlbuf.at[z], m_send, m_recv, "kv")
    w_copies = spread(lambda peer: wsend.at[lax.rem(peer, 4)], wbuf.at[z], w_send, w_recv, "kv")
    arrive(m_copies)
    ml = jnp.concatenate([mlbuf[j] for j in range(KV)], axis=0)
    shares = jnp.exp(ml - jnp.max(ml, axis=0, keepdims=True))
    grand = jnp.sum(shares * pltpu.roll(ml, half, 1), axis=0, keepdims=True)
    in_use = iota(ml.shape, 1) < quarter
    shares = jnp.where(in_use, shares / jnp.where(in_use[0:1], grand, 1.0), 0.0)
    columns = jnp.transpose(shares)
    arrive(w_copies)
    attended = columns[0:quarter, 0:1] * wbuf[0].astype(F32)
    for j in range(1, KV):
        attended = attended + columns[0:quarter, j : j + 1] * wbuf[j].astype(F32)
    ld_lam.wait()
    ld_hg.wait()
    lambdas = lam[0:1, 0:1]
    for g in range(1, heads):
        lambdas = jnp.where(
            lax.rem(iota((quarter, 1), 0), maps) // 2 == g, lam[0:1, g : g + 1], lambdas
        )
    diff = attended - lambdas * pltpu.roll(attended, quarter - 1, 0)
    normed = (
        diff
        * lax.rsqrt(jnp.mean(diff * diff, axis=1, keepdims=True) + EPS)
        * hg[...].astype(F32)
    ).astype(BF16)
    nbuf[mine] = normed
    arrive(spread(lambda peer: nbuf.at[mine], nbuf.at[mine], n_send, n_recv, "kv", (2, 1, KV - 1)))
    normed = jnp.concatenate([nbuf[c] for c in range(4)], axis=0)
    outs = []
    for g in range(heads):
        pick = iota((rows, lines), 1) == iota((rows, lines), 0) * maps + 2 * g
        outs.append(dot(pick.astype(BF16), normed))
    heads_out = jnp.concatenate(outs, axis=1).astype(BF16)
    ld_wo.wait()
    dbuf[t] = dot(heads_out, wo[...])
    arrive(spread(lambda peer: dbuf.at[t], dbuf.at[t], d_send, d_recv, "tp"))
    projected = dbuf[0]
    for j in range(1, TP):
        projected = projected + dbuf[j]
    mixed = (block + projected).astype(BF16).astype(F32)
    sqbuf[z] = to_lanes(jnp.sum(mixed * mixed, axis=1, keepdims=True))
    s_copies = spread(lambda peer: sqbuf.at[z], sqbuf.at[z], s_send, s_recv, "kv")
    ld_mg.wait()
    gain2 = jnp.concatenate([mg[k : k + 1, :] for k in range(width // LANES)], axis=1).astype(F32)
    scaled2 = (mixed * gain2).astype(BF16)
    ld_wu.wait()
    up = dot(scaled2, wu[...])
    owners = KV // 2
    owned = lax.rem(z, owners)
    share_width = up.shape[1] // owners
    for j in range(owners):
        us[j] = up[:, j * share_width : (j + 1) * share_width].astype(BF16)
    ur[z] = us[owned]
    u_copies = spread(lambda peer: us.at[lax.rem(peer, owners)], ur.at[z], u_send, u_recv, "kv")
    arrive(s_copies)
    square2 = sqbuf[0]
    for j in range(1, KV):
        square2 = square2 + sqbuf[j]
    inv2 = to_rows(lax.rsqrt(square2 / D + EPS), rows)
    arrive(u_copies)
    up_sum = ur[0].astype(F32)
    for j in range(1, KV):
        up_sum = up_sum + ur[j].astype(F32)
    act = jnp.maximum(inv2 * up_sum, 0.0)
    hbuf[owned] = (act * act).astype(BF16)
    near = [owners // 2]
    for d in range(owners // 2 - 1, 0, -1):
        near += [d, KV - d]
    arrive(spread(lambda peer: hbuf.at[owned], hbuf.at[owned], h_send, h_recv, "kv", near))
    hidden = jnp.concatenate([hbuf[j] for j in range(owners)], axis=1)
    ld_wd.wait()
    down = dot(hidden, wd[...])
    for k in range(width // LANES):
        fs[k] = down[:, k * LANES : (k + 1) * LANES]
    fr[t] = fs[t // per_tile]
    earlier = len(started)
    f_copies = spread(lambda peer: fs.at[peer // per_tile], fr.at[t], f_send, f_recv, "tp")
    for copy in started[:earlier]:
        copy.wait_send()
    arrive(f_copies)
    y = fr[0]
    for j in range(1, TP):
        y = y + fr[j]
    for k in range(width // LANES):
        y = y + jnp.where(t // per_tile == k, mixed[:, k * LANES : (k + 1) * LANES], 0.0)
    result = y[:, 0:piece]
    for k in range(1, per_tile):
        result = jnp.where(lax.rem(t, per_tile) == k, y[:, k * piece : (k + 1) * piece], result)
    out_ref[...] = result.astype(out_ref.dtype)
    for copy in f_copies:
        copy.wait_send()


def body(
    KV,
    TP,
    residual,
    cache_keys,
    cache_values,
    norm_gain,
    query_weight,
    key_weight,
    value_weight,
    head_lambda,
    head_gain,
    out_weight,
    mixer_gain,
    up_weight,
    down_weight,
):
    rows, piece = residual.shape
    positions, depth = cache_keys.shape[1], cache_keys.shape[3]
    width = out_weight.shape[1]
    qcols = query_weight.shape[1]
    lines = rows * qcols * 2 // LANES
    share = up_weight.shape[1] * 2 // KV
    any_spec = pl.BlockSpec(memory_space=pl.ANY)
    dma = pltpu.SemaphoreType.DMA
    keys = cache_keys.reshape(rows, positions, depth)
    values = cache_values.reshape(rows, positions, depth)
    args = (
        residual,
        keys,
        values,
        norm_gain.reshape(width // LANES, LANES),
        query_weight,
        key_weight,
        value_weight,
        head_lambda.reshape(1, -1),
        head_gain.reshape(1, -1),
        out_weight,
        mixer_gain.reshape(width // LANES, LANES),
        up_weight,
        down_weight,
    )
    kv_sems = [dma((KV - 1,))] * 2
    tp_sems = [dma((TP - 1,))] * 2
    return pl.pallas_call(
        functools.partial(kernel, KV, TP),
        out_shape=jax.ShapeDtypeStruct((rows, piece), residual.dtype),
        in_specs=[any_spec] * len(args),
        out_specs=pl.BlockSpec(memory_space=pltpu.VMEM),
        scratch_shapes=[
            pltpu.VMEM((rows, piece), BF16),
            pltpu.VMEM(keys.shape, BF16),
            pltpu.VMEM(values.shape, BF16),
            pltpu.VMEM((width // LANES, LANES), BF16),
            pltpu.VMEM((width, qcols + 2 * LANES), BF16),
            pltpu.VMEM((1, head_lambda.shape[0]), F32),
            pltpu.VMEM((1, head_gain.shape[0]), BF16),
            pltpu.VMEM(out_weight.shape, BF16),
            pltpu.VMEM((width // LANES, LANES), BF16),
            pltpu.VMEM(up_weight.shape, BF16),
            pltpu.VMEM(down_weight.shape, BF16),
            pltpu.VMEM((TP, rows, LANES), BF16),
            pltpu.VMEM((KV, rows, qcols), BF16),
            pltpu.VMEM((KV, 1, 3 * LANES), F32),
            pltpu.VMEM((KV, 1, 3 * LANES), F32),
            pltpu.VMEM((4, lines // 4, LANES), BF16),
            pltpu.VMEM((KV, lines // 4, LANES), BF16),
            pltpu.VMEM((4, 1, LANES), F32),
            pltpu.VMEM((KV, 1, LANES), F32),
            pltpu.VMEM((4, lines // 4, LANES), BF16),
            pltpu.VMEM((TP, rows, width), F32),
            pltpu.VMEM((KV, 1, LANES), F32),
            pltpu.VMEM((KV // 2, rows, share), BF16),
            pltpu.VMEM((KV, rows, share), BF16),
            pltpu.VMEM((KV // 2, rows, share), BF16),
            pltpu.VMEM((width // LANES, rows, LANES), F32),
            pltpu.VMEM((TP, rows, LANES), F32),
            pltpu.SemaphoreType.REGULAR((3,)),
            dma((13,)),
            *tp_sems,
            *kv_sems,
            *kv_sems,
            *kv_sems,
            *kv_sems,
            *kv_sems,
            *tp_sems,
            *kv_sems,
            *kv_sems,
            *kv_sems,
            *tp_sems,
        ],
        compiler_params=pltpu.CompilerParams(
            collective_id=0, has_side_effects=True, vmem_limit_bytes=64 * 1000 * 1000
        ),
        name="layer",
    )(*args)


def solution(mesh):
    in_specs = (
        P("grp", ("kv", "tp")),
        P("grp", "kv", "tp", None),
        P("grp", "kv", "tp", None),
        P("kv"),
        P("kv", "tp"),
        P("kv", "tp"),
        P("kv", "tp"),
        P("tp"),
        P(),
        P("tp", "kv"),
        P("kv"),
        P("kv", "tp"),
        P("tp", "kv"),
    )
    out_specs = P("grp", ("kv", "tp"))
    fn = functools.partial(body, mesh.shape["kv"], mesh.shape["tp"])
    return jax.shard_map(fn, mesh=mesh, in_specs=in_specs, out_specs=out_specs, check_vma=False)
```

```python
import functools

import jax
import jax.numpy as jnp
from jax import lax
from jax.experimental import pallas as pl
from jax.experimental.pallas import tpu as pltpu
from jax.sharding import PartitionSpec as P

EPS = 1e-06
MESH = pl.DeviceIdType.MESH
F32 = jnp.float32
BF16 = jnp.bfloat16
LANES = 128
LOW = -1e30


def far_first(n):
    order = [n // 2]
    for k in range(1, n // 2 + 1):
        for d in (n // 2 - k, n // 2 + k):
            if 0 < d < n:
                order.append(d)
    return order


def iota(shape, dim):
    return lax.broadcasted_iota(jnp.int32, shape, dim)


def dot(a, b):
    return jnp.dot(a, b, preferred_element_type=F32)


def to_lanes(column):
    wide = jnp.broadcast_to(column, (column.shape[0], LANES))
    diagonal = iota(wide.shape, 0) == iota(wide.shape, 1)
    return jnp.sum(jnp.where(diagonal, wide, 0.0), axis=0, keepdims=True)


def to_rows(row, rows):
    wide = jnp.broadcast_to(row, (rows, LANES))
    diagonal = iota(wide.shape, 0) == iota(wide.shape, 1)
    return jnp.sum(jnp.where(diagonal, wide, 0.0), axis=1, keepdims=True)


def kernel(
    KV,
    TP,
    res_h,
    keys_h,
    values_h,
    ng_h,
    wq_h,
    wk_h,
    wv_h,
    lam_h,
    hg_h,
    wo_h,
    mg_h,
    wu_h,
    wd_h,
    out_ref,
    res,
    keys,
    values,
    ng,
    wp,
    lam,
    hg,
    wo,
    mg,
    wu,
    wd,
    abuf,
    qbuf,
    kvs,
    kvr,
    lined_s,
    wsend,
    wbuf,
    mlsend,
    mlbuf,
    nbuf,
    dbuf,
    sqbuf,
    us,
    ur,
    hbuf,
    fs,
    fr,
    ring_sem,
    load_sem,
    a_send,
    a_recv,
    q_send,
    q_recv,
    r_send,
    r_recv,
    w_send,
    w_recv,
    m_send,
    m_recv,
    n_send,
    n_recv,
    d_send,
    d_recv,
    s_send,
    s_recv,
    u_send,
    u_recv,
    h_send,
    h_recv,
    f_send,
    f_recv,
):
    z = lax.axis_index("kv")
    t = lax.axis_index("tp")
    rows = res_h.shape[0]
    piece = res_h.shape[1]
    per_tile = LANES // piece
    width = wo.shape[1]
    D = KV * width
    qcols = wq_h.shape[1]
    heads = qcols // LANES
    half = LANES // 2
    maps = heads * 2
    lines = rows * maps

    def load(src, dst, k):
        copy = pltpu.make_async_copy(src, dst, load_sem.at[k])
        copy.start()
        return copy

    ld_res = load(res_h, res, 0)
    barrier = pltpu.get_barrier_semaphore()
    for u in range(1, TP):
        peer = lax.rem(t + u, TP)
        pl.semaphore_signal(barrier, inc=1, device_id={"tp": peer}, device_id_type=MESH)

    def both_ways(sem, d):
        for u in (d, KV - d):
            peer = lax.rem(z + u, KV)
            pl.semaphore_signal(sem, inc=1, device_id={"kv": peer}, device_id_type=MESH)

    both_ways(barrier, 1)
    both_ways(barrier, 2)
    ld_ng = load(ng_h, ng, 1)
    ld_wq = load(wq_h, wp.at[:, 0:qcols], 2)
    ld_wk = load(wk_h, wp.at[:, qcols : qcols + LANES], 3)
    ld_wv = load(wv_h, wp.at[:, qcols + LANES : qcols + 2 * LANES], 4)

    started = []

    def send(src, dst, ssem, rsem, axis, peer):
        copy = pltpu.make_async_remote_copy(
            src_ref=src,
            dst_ref=dst,
            send_sem=ssem,
            recv_sem=rsem,
            device_id={axis: peer},
            device_id_type=MESH,
        )
        copy.start()
        started.append(copy)
        return copy

    kv_order = far_first(KV)
    tp_order = far_first(TP)

    def spread(src_of, dst, sems, rsems, axis, order=None):
        me, n = (z, KV) if axis == "kv" else (t, TP)
        if order is None:
            order = kv_order if axis == "kv" else tp_order
        copies = []
        for d in order:
            peer = lax.rem(me + d, n)
            copies.append(send(src_of(peer), dst, sems.at[d - 1], rsems.at[d - 1], axis, peer))
        return copies

    def arrive(copies):
        for copy in copies:
            copy.wait_recv()

    ld_res.wait()
    own_piece = res[...].astype(F32)
    tiled = jnp.concatenate([own_piece] * per_tile, axis=1)
    at = iota(tiled.shape, 1) // piece == lax.rem(t, per_tile)
    abuf[t] = jnp.where(at, tiled, 0.0).astype(BF16)
    pl.semaphore_wait(barrier, TP - 1 + 4)
    a_copies = spread(lambda peer: abuf.at[t], abuf.at[t], a_send, a_recv, "tp")
    both_ways(ring_sem.at[0], 2)
    pl.semaphore_wait(ring_sem.at[0], 2)
    both_ways(ring_sem.at[1], 4)
    arrive(a_copies)
    block = jnp.concatenate(
        [
            sum(abuf[k * per_tile + j].astype(F32) for j in range(per_tile))
            for k in range(TP // per_tile)
        ],
        axis=1,
    )
    ld_ng.wait()
    gain = jnp.concatenate([ng[k : k + 1, :] for k in range(width // LANES)], axis=1).astype(F32)
    scaled = (block * gain).astype(BF16)
    ld_wq.wait()
    ld_wk.wait()
    ld_wv.wait()
    proj = dot(scaled, wp[...])
    qbuf[z] = proj[:, 0:qcols].astype(BF16)
    square = to_lanes(jnp.sum(block * block, axis=1, keepdims=True))
    for j in range(KV):
        kvs[j] = jnp.concatenate([proj[j : j + 1, qcols:], square], axis=1)
    kvr[z] = kvs[z]
    pl.semaphore_wait(ring_sem.at[1], 2)
    q_copies = spread(lambda peer: qbuf.at[z], qbuf.at[z], q_send, q_recv, "kv")
    r_copies = spread(lambda peer: kvs.at[peer], kvr.at[z], r_send, r_recv, "kv")
    ld_keys = load(keys_h, keys, 5)
    ld_values = load(values_h, values, 6)
    ld_lam = load(lam_h, lam, 7)
    ld_hg = load(hg_h, hg, 8)
    ld_wo = load(wo_h, wo, 9)
    ld_mg = load(mg_h, mg, 10)
    ld_wu = load(wu_h, wu, 11)
    ld_wd = load(wd_h, wd, 12)
    arrive(q_copies)
    arrive(r_copies)
    q_sum = qbuf[0].astype(F32)
    r_sum = kvr[0]
    for j in range(1, KV):
        q_sum = q_sum + qbuf[j].astype(F32)
        r_sum = r_sum + kvr[j]
    inv_lanes = lax.rsqrt(r_sum[:, 2 * LANES :] / D + EPS)
    inv_own = jnp.sum(
        jnp.where(iota(inv_lanes.shape, 1) == z, inv_lanes, 0.0), axis=1, keepdims=True
    )
    new_key = (inv_own * r_sum[:, 0:LANES]).astype(BF16).astype(F32)
    new_value = (inv_own * r_sum[:, LANES : 2 * LANES]).astype(BF16).astype(F32)
    query = (to_rows(inv_lanes, rows) * q_sum).astype(BF16)

    lane = iota((rows, LANES), 1)
    for g in range(heads):
        head = query[:, g * LANES : (g + 1) * LANES].astype(F32) * (1.0 / half**0.5)
        for c in range(2):
            lined_s[pl.ds(2 * g + c, rows, stride=maps), :] = jnp.where(lane // half == c, head, 0.0)
    lined = lined_s[...]

    ld_keys.wait()
    ld_values.wait()
    tops, totals, sums = [], [], []
    for p in range(lines // 8):
        seqs = 8 // maps
        qp = lined[8 * p : 8 * p + 8, :].astype(BF16)
        scores = None
        for k in range(seqs):
            part = lax.dot_general(
                qp, keys[seqs * p + k], (((1,), (1,)), ((), ())), preferred_element_type=F32
            )
            if scores is None:
                scores = part
            else:
                scores = jnp.where(iota(part.shape, 0) // maps == k, part, scores)
        top = jnp.max(scores, axis=1, keepdims=True)
        expo = jnp.exp(scores - top)
        total = jnp.sum(expo, axis=1, keepdims=True)
        probs = expo.astype(BF16)
        weighted = None
        for k in range(seqs):
            part = dot(probs, values[seqs * p + k])
            if weighted is None:
                weighted = part
            else:
                weighted = jnp.where(iota(part.shape, 0) // maps == k, part, weighted)
        tops.append(top)
        totals.append(total)
        sums.append(weighted)
    top = jnp.concatenate(tops, axis=0)
    total = jnp.concatenate(totals, axis=0)
    weighted = jnp.concatenate(sums, axis=0)
    own = jnp.sum(lined * new_key, axis=1, keepdims=True)
    own = jnp.where(iota(own.shape, 0) // maps == z, own, LOW)
    new_top = jnp.maximum(top, own)
    old_part = jnp.exp(top - new_top)
    own_part = jnp.exp(own - new_top)
    total = total * old_part + own_part
    weighted = weighted * old_part + own_part * new_value
    quarter = lines // 4
    mine = lax.rem(z, 4)
    lane = iota((quarter, LANES), 1)
    line = iota((quarter, LANES), 0)
    for c in range(4):
        at = slice(c * quarter, (c + 1) * quarter)
        wsend[c] = weighted[at].astype(BF16)
        both = jnp.where(lane == line, new_top[at], jnp.where(lane == line + half, total[at], 0.0))
        mlsend[c] = jnp.sum(both, axis=0, keepdims=True)
    wbuf[z] = wsend[mine]
    mlbuf[z] = mlsend[mine]
    m_copies = spread(lambda peer: mlsend.at[lax.rem(peer, 4)], mlbuf.at[z], m_send, m_recv, "kv")
    w_copies = spread(lambda peer: wsend.at[lax.rem(peer, 4)], wbuf.at[z], w_send, w_recv, "kv")
    arrive(m_copies)
    ml = jnp.concatenate([mlbuf[j] for j in range(KV)], axis=0)
    shares = jnp.exp(ml - jnp.max(ml, axis=0, keepdims=True))
    grand = jnp.sum(shares * pltpu.roll(ml, half, 1), axis=0, keepdims=True)
    in_use = iota(ml.shape, 1) < quarter
    shares = jnp.where(in_use, shares / jnp.where(in_use[0:1], grand, 1.0), 0.0)
    columns = jnp.transpose(shares)
    arrive(w_copies)
    attended = columns[0:quarter, 0:1] * wbuf[0].astype(F32)
    for j in range(1, KV):
        attended = attended + columns[0:quarter, j : j + 1] * wbuf[j].astype(F32)
    ld_lam.wait()
    ld_hg.wait()
    lambdas = lam[0:1, 0:1]
    for g in range(1, heads):
        lambdas = jnp.where(
            lax.rem(iota((quarter, 1), 0), maps) // 2 == g, lam[0:1, g : g + 1], lambdas
        )
    diff = attended - lambdas * pltpu.roll(attended, quarter - 1, 0)
    normed = (
        diff
        * lax.rsqrt(jnp.mean(diff * diff, axis=1, keepdims=True) + EPS)
        * hg[...].astype(F32)
    ).astype(BF16)
    nbuf[mine] = normed
    arrive(spread(lambda peer: nbuf.at[mine], nbuf.at[mine], n_send, n_recv, "kv", (2, 1, KV - 1)))
    for c in range(4):
        lined_s[c * quarter : (c + 1) * quarter, :] = nbuf[c].astype(F32)
    outs = [lined_s[pl.ds(2 * g, rows, stride=maps), :] for g in range(heads)]
    heads_out = jnp.concatenate(outs, axis=1).astype(BF16)
    ld_wo.wait()
    dbuf[t] = dot(heads_out, wo[...])
    arrive(spread(lambda peer: dbuf.at[t], dbuf.at[t], d_send, d_recv, "tp"))
    projected = dbuf[0]
    for j in range(1, TP):
        projected = projected + dbuf[j]
    mixed = (block + projected).astype(BF16).astype(F32)
    sqbuf[z] = to_lanes(jnp.sum(mixed * mixed, axis=1, keepdims=True))
    s_copies = spread(lambda peer: sqbuf.at[z], sqbuf.at[z], s_send, s_recv, "kv")
    ld_mg.wait()
    gain2 = jnp.concatenate([mg[k : k + 1, :] for k in range(width // LANES)], axis=1).astype(F32)
    scaled2 = (mixed * gain2).astype(BF16)
    ld_wu.wait()
    up = dot(scaled2, wu[...])
    owners = KV // 2
    owned = lax.rem(z, owners)
    share_width = up.shape[1] // owners
    for j in range(owners):
        us[j] = up[:, j * share_width : (j + 1) * share_width].astype(BF16)
    ur[z] = us[owned]
    u_copies = spread(lambda peer: us.at[lax.rem(peer, owners)], ur.at[z], u_send, u_recv, "kv")
    arrive(s_copies)
    square2 = sqbuf[0]
    for j in range(1, KV):
        square2 = square2 + sqbuf[j]
    inv2 = to_rows(lax.rsqrt(square2 / D + EPS), rows)
    arrive(u_copies)
    up_sum = ur[0].astype(F32)
    for j in range(1, KV):
        up_sum = up_sum + ur[j].astype(F32)
    act = jnp.maximum(inv2 * up_sum, 0.0)
    hbuf[owned] = (act * act).astype(BF16)
    near = [owners // 2]
    for d in range(owners // 2 - 1, 0, -1):
        near += [d, KV - d]
    arrive(spread(lambda peer: hbuf.at[owned], hbuf.at[owned], h_send, h_recv, "kv", near))
    hidden = jnp.concatenate([hbuf[j] for j in range(owners)], axis=1)
    ld_wd.wait()
    down = dot(hidden, wd[...])
    for k in range(width // LANES):
        fs[k] = down[:, k * LANES : (k + 1) * LANES]
    fr[t] = fs[t // per_tile]
    earlier = len(started)
    f_copies = spread(lambda peer: fs.at[peer // per_tile], fr.at[t], f_send, f_recv, "tp")
    for copy in started[:earlier]:
        copy.wait_send()
    arrive(f_copies)
    y = fr[0]
    for j in range(1, TP):
        y = y + fr[j]
    for k in range(width // LANES):
        y = y + jnp.where(t // per_tile == k, mixed[:, k * LANES : (k + 1) * LANES], 0.0)
    result = y[:, 0:piece]
    for k in range(1, per_tile):
        result = jnp.where(lax.rem(t, per_tile) == k, y[:, k * piece : (k + 1) * piece], result)
    out_ref[...] = result.astype(out_ref.dtype)
    for copy in f_copies:
        copy.wait_send()


def body(
    KV,
    TP,
    residual,
    cache_keys,
    cache_values,
    norm_gain,
    query_weight,
    key_weight,
    value_weight,
    head_lambda,
    head_gain,
    out_weight,
    mixer_gain,
    up_weight,
    down_weight,
):
    rows, piece = residual.shape
    positions, depth = cache_keys.shape[1], cache_keys.shape[3]
    width = out_weight.shape[1]
    qcols = query_weight.shape[1]
    lines = rows * qcols * 2 // LANES
    share = up_weight.shape[1] * 2 // KV
    any_spec = pl.BlockSpec(memory_space=pl.ANY)
    dma = pltpu.SemaphoreType.DMA
    keys = cache_keys.reshape(rows, positions, depth)
    values = cache_values.reshape(rows, positions, depth)
    args = (
        residual,
        keys,
        values,
        norm_gain.reshape(width // LANES, LANES),
        query_weight,
        key_weight,
        value_weight,
        head_lambda.reshape(1, -1),
        head_gain.reshape(1, -1),
        out_weight,
        mixer_gain.reshape(width // LANES, LANES),
        up_weight,
        down_weight,
    )
    kv_sems = [dma((KV - 1,))] * 2
    tp_sems = [dma((TP - 1,))] * 2
    return pl.pallas_call(
        functools.partial(kernel, KV, TP),
        out_shape=jax.ShapeDtypeStruct((rows, piece), residual.dtype),
        in_specs=[any_spec] * len(args),
        out_specs=pl.BlockSpec(memory_space=pltpu.VMEM),
        scratch_shapes=[
            pltpu.VMEM((rows, piece), BF16),
            pltpu.VMEM(keys.shape, BF16),
            pltpu.VMEM(values.shape, BF16),
            pltpu.VMEM((width // LANES, LANES), BF16),
            pltpu.VMEM((width, qcols + 2 * LANES), BF16),
            pltpu.VMEM((1, head_lambda.shape[0]), F32),
            pltpu.VMEM((1, head_gain.shape[0]), BF16),
            pltpu.VMEM(out_weight.shape, BF16),
            pltpu.VMEM((width // LANES, LANES), BF16),
            pltpu.VMEM(up_weight.shape, BF16),
            pltpu.VMEM(down_weight.shape, BF16),
            pltpu.VMEM((TP, rows, LANES), BF16),
            pltpu.VMEM((KV, rows, qcols), BF16),
            pltpu.VMEM((KV, 1, 3 * LANES), F32),
            pltpu.VMEM((KV, 1, 3 * LANES), F32),
            pltpu.VMEM((lines, LANES), F32),
            pltpu.VMEM((4, lines // 4, LANES), BF16),
            pltpu.VMEM((KV, lines // 4, LANES), BF16),
            pltpu.VMEM((4, 1, LANES), F32),
            pltpu.VMEM((KV, 1, LANES), F32),
            pltpu.VMEM((4, lines // 4, LANES), BF16),
            pltpu.VMEM((TP, rows, width), F32),
            pltpu.VMEM((KV, 1, LANES), F32),
            pltpu.VMEM((KV // 2, rows, share), BF16),
            pltpu.VMEM((KV, rows, share), BF16),
            pltpu.VMEM((KV // 2, rows, share), BF16),
            pltpu.VMEM((width // LANES, rows, LANES), F32),
            pltpu.VMEM((TP, rows, LANES), F32),
            pltpu.SemaphoreType.REGULAR((2,)),
            dma((13,)),
            *tp_sems,
            *kv_sems,
            *kv_sems,
            *kv_sems,
            *kv_sems,
            *kv_sems,
            *tp_sems,
            *kv_sems,
            *kv_sems,
            *kv_sems,
            *tp_sems,
        ],
        compiler_params=pltpu.CompilerParams(
            collective_id=0, has_side_effects=True, vmem_limit_bytes=64 * 1000 * 1000
        ),
        name="layer",
    )(*args)


def solution(mesh):
    in_specs = (
        P("grp", ("kv", "tp")),
        P("grp", "kv", "tp", None),
        P("grp", "kv", "tp", None),
        P("kv"),
        P("kv", "tp"),
        P("kv", "tp"),
        P("kv", "tp"),
        P("tp"),
        P(),
        P("tp", "kv"),
        P("kv"),
        P("kv", "tp"),
        P("tp", "kv"),
    )
    out_specs = P("grp", ("kv", "tp"))
    fn = functools.partial(body, mesh.shape["kv"], mesh.shape["tp"])
    return jax.shard_map(fn, mesh=mesh, in_specs=in_specs, out_specs=out_specs, check_vma=False)
```

```python
import functools

import jax
import jax.numpy as jnp
from jax import lax
from jax.experimental import pallas as pl
from jax.experimental.pallas import tpu as pltpu
from jax.sharding import PartitionSpec as P

EPS = 1e-06
MESH = pl.DeviceIdType.MESH
F32 = jnp.float32
BF16 = jnp.bfloat16
LANES = 128
LOW = -1e30


def far_first(n):
    def distance(k):
        odd = lax.rem(k, 2)
        return n // 2 + odd * ((k + 1) // 2) - (1 - odd) * (k // 2)

    return distance


def loop(n, step):
    def run(k, carry):
        step(k)
        return carry

    lax.fori_loop(0, n, run, 0)


class Spread:
    def __init__(self, copy_to, distances, steps):
        self.copy_to, self.distances, self.steps = copy_to, distances, steps

    def each(self, act):
        if self.steps is None:
            for d in self.distances:
                act(self.copy_to(d))
        else:
            loop(self.steps, lambda k: act(self.copy_to(self.distances(k))))

    def start(self):
        self.each(lambda copy: copy.start())
        return self

    def arrive(self):
        self.each(lambda copy: copy.wait_recv())

    def sent(self):
        self.each(lambda copy: copy.wait_send())


def iota(shape, dim):
    return lax.broadcasted_iota(jnp.int32, shape, dim)


def dot(a, b):
    return jnp.dot(a, b, preferred_element_type=F32)


def to_lanes(column):
    wide = jnp.broadcast_to(column, (column.shape[0], LANES))
    diagonal = iota(wide.shape, 0) == iota(wide.shape, 1)
    return jnp.sum(jnp.where(diagonal, wide, 0.0), axis=0, keepdims=True)


def to_rows(row, rows):
    wide = jnp.broadcast_to(row, (rows, LANES))
    diagonal = iota(wide.shape, 0) == iota(wide.shape, 1)
    return jnp.sum(jnp.where(diagonal, wide, 0.0), axis=1, keepdims=True)


def kernel(
    KV,
    TP,
    res_h,
    keys_h,
    values_h,
    ng_h,
    wq_h,
    wk_h,
    wv_h,
    lam_h,
    hg_h,
    wo_h,
    mg_h,
    wu_h,
    wd_h,
    out_ref,
    res,
    keys,
    values,
    ng,
    wp,
    lam,
    hg,
    wo,
    mg,
    wu,
    wd,
    abuf,
    qbuf,
    kvs,
    kvr,
    lined_s,
    wsend,
    wbuf,
    mlsend,
    mlbuf,
    nbuf,
    dbuf,
    sqbuf,
    us,
    ur,
    hbuf,
    fs,
    fr,
    ring_sem,
    load_sem,
    a_send,
    a_recv,
    q_send,
    q_recv,
    r_send,
    r_recv,
    w_send,
    w_recv,
    m_send,
    m_recv,
    n_send,
    n_recv,
    d_send,
    d_recv,
    s_send,
    s_recv,
    u_send,
    u_recv,
    h_send,
    h_recv,
    f_send,
    f_recv,
):
    z = lax.axis_index("kv")
    t = lax.axis_index("tp")
    rows = res_h.shape[0]
    piece = res_h.shape[1]
    per_tile = LANES // piece
    width = wo.shape[1]
    D = KV * width
    qcols = wq_h.shape[1]
    heads = qcols // LANES
    half = LANES // 2
    maps = heads * 2
    lines = rows * maps

    def load(src, dst, k):
        copy = pltpu.make_async_copy(src, dst, load_sem.at[k])
        copy.start()
        return copy

    ld_res = load(res_h, res, 0)
    barrier = pltpu.get_barrier_semaphore()
    def greet(k):
        peer = lax.rem(t + k + 1, TP)
        pl.semaphore_signal(barrier, inc=1, device_id={"tp": peer}, device_id_type=MESH)

    loop(TP - 1, greet)

    def both_ways(sem, d):
        for u in (d, KV - d):
            peer = lax.rem(z + u, KV)
            pl.semaphore_signal(sem, inc=1, device_id={"kv": peer}, device_id_type=MESH)

    both_ways(barrier, 1)
    both_ways(barrier, 2)
    ld_ng = load(ng_h, ng, 1)
    ld_wq = load(wq_h, wp.at[:, 0:qcols], 2)
    ld_wk = load(wk_h, wp.at[:, qcols : qcols + LANES], 3)
    ld_wv = load(wv_h, wp.at[:, qcols + LANES : qcols + 2 * LANES], 4)

    started = []

    def spread(src_of, dst, ssem, rsem, axis, distances=None):
        me, n = (z, KV) if axis == "kv" else (t, TP)

        def copy_to(d):
            peer = lax.rem(me + d, n)
            return pltpu.make_async_remote_copy(
                src_ref=src_of(peer),
                dst_ref=dst,
                send_sem=ssem.at[d - 1],
                recv_sem=rsem.at[d - 1],
                device_id={axis: peer},
                device_id_type=MESH,
            )

        if distances is None:
            out = Spread(copy_to, far_first(n), n - 1)
        else:
            out = Spread(copy_to, distances, None)
        started.append(out)
        return out

    def start_both(first, second):
        def step(k):
            d = first.distances(k)
            first.copy_to(d).start()
            second.copy_to(d).start()

        loop(first.steps, step)

    ld_res.wait()
    own_piece = res[...].astype(F32)
    tiled = jnp.concatenate([own_piece] * per_tile, axis=1)
    at = iota(tiled.shape, 1) // piece == lax.rem(t, per_tile)
    abuf[t] = jnp.where(at, tiled, 0.0).astype(BF16)
    pl.semaphore_wait(barrier, TP - 1 + 4)
    a_copies = spread(lambda peer: abuf.at[t], abuf.at[t], a_send, a_recv, "tp").start()
    both_ways(ring_sem.at[0], 2)
    pl.semaphore_wait(ring_sem.at[0], 2)
    both_ways(ring_sem.at[1], 4)
    a_copies.arrive()
    block = jnp.concatenate(
        [
            sum(abuf[k * per_tile + j].astype(F32) for j in range(per_tile))
            for k in range(TP // per_tile)
        ],
        axis=1,
    )
    ld_ng.wait()
    gain = jnp.concatenate([ng[k : k + 1, :] for k in range(width // LANES)], axis=1).astype(F32)
    scaled = (block * gain).astype(BF16)
    ld_wq.wait()
    ld_wk.wait()
    ld_wv.wait()
    proj = dot(scaled, wp[...])
    qbuf[z] = proj[:, 0:qcols].astype(BF16)
    square = to_lanes(jnp.sum(block * block, axis=1, keepdims=True))
    for j in range(KV):
        kvs[j] = jnp.concatenate([proj[j : j + 1, qcols:], square], axis=1)
    kvr[z] = kvs[z]
    pl.semaphore_wait(ring_sem.at[1], 2)
    q_copies = spread(lambda peer: qbuf.at[z], qbuf.at[z], q_send, q_recv, "kv")
    r_copies = spread(lambda peer: kvs.at[peer], kvr.at[z], r_send, r_recv, "kv")

    start_both(r_copies, q_copies)
    ld_keys = load(keys_h, keys, 5)
    ld_values = load(values_h, values, 6)
    ld_lam = load(lam_h, lam, 7)
    ld_hg = load(hg_h, hg, 8)
    ld_wo = load(wo_h, wo, 9)
    ld_mg = load(mg_h, mg, 10)
    ld_wu = load(wu_h, wu, 11)
    ld_wd = load(wd_h, wd, 12)
    q_copies.arrive()
    r_copies.arrive()
    q_sum = qbuf[0].astype(F32)
    r_sum = kvr[0]
    for j in range(1, KV):
        q_sum = q_sum + qbuf[j].astype(F32)
        r_sum = r_sum + kvr[j]
    inv_lanes = lax.rsqrt(r_sum[:, 2 * LANES :] / D + EPS)
    inv_own = jnp.sum(
        jnp.where(iota(inv_lanes.shape, 1) == z, inv_lanes, 0.0), axis=1, keepdims=True
    )
    new_key = (inv_own * r_sum[:, 0:LANES]).astype(BF16).astype(F32)
    new_value = (inv_own * r_sum[:, LANES : 2 * LANES]).astype(BF16).astype(F32)
    query = (to_rows(inv_lanes, rows) * q_sum).astype(BF16)

    lane = iota((rows, LANES), 1)
    for g in range(heads):
        head = query[:, g * LANES : (g + 1) * LANES].astype(F32) * (1.0 / half**0.5)
        for c in range(2):
            lined_s[pl.ds(2 * g + c, rows, stride=maps), :] = jnp.where(lane // half == c, head, 0.0)
    lined = lined_s[...]

    ld_keys.wait()
    ld_values.wait()
    tops, totals, sums = [], [], []
    for p in range(lines // 8):
        seqs = 8 // maps
        qp = lined[8 * p : 8 * p + 8, :].astype(BF16)
        scores = None
        for k in range(seqs):
            part = lax.dot_general(
                qp, keys[seqs * p + k], (((1,), (1,)), ((), ())), preferred_element_type=F32
            )
            if scores is None:
                scores = part
            else:
                scores = jnp.where(iota(part.shape, 0) // maps == k, part, scores)
        top = jnp.max(scores, axis=1, keepdims=True)
        expo = jnp.exp(scores - top)
        total = jnp.sum(expo, axis=1, keepdims=True)
        probs = expo.astype(BF16)
        weighted = None
        for k in range(seqs):
            part = dot(probs, values[seqs * p + k])
            if weighted is None:
                weighted = part
            else:
                weighted = jnp.where(iota(part.shape, 0) // maps == k, part, weighted)
        tops.append(top)
        totals.append(total)
        sums.append(weighted)
    top = jnp.concatenate(tops, axis=0)
    total = jnp.concatenate(totals, axis=0)
    weighted = jnp.concatenate(sums, axis=0)
    own = jnp.sum(lined * new_key, axis=1, keepdims=True)
    own = jnp.where(iota(own.shape, 0) // maps == z, own, LOW)
    new_top = jnp.maximum(top, own)
    old_part = jnp.exp(top - new_top)
    own_part = jnp.exp(own - new_top)
    total = total * old_part + own_part
    weighted = weighted * old_part + own_part * new_value
    quarter = lines // 4
    mine = lax.rem(z, 4)
    lane = iota((quarter, LANES), 1)
    line = iota((quarter, LANES), 0)
    for c in range(4):
        at = slice(c * quarter, (c + 1) * quarter)
        wsend[c] = weighted[at].astype(BF16)
        both = jnp.where(lane == line, new_top[at], jnp.where(lane == line + half, total[at], 0.0))
        mlsend[c] = jnp.sum(both, axis=0, keepdims=True)
    wbuf[z] = wsend[mine]
    mlbuf[z] = mlsend[mine]
    m_copies = spread(lambda peer: mlsend.at[lax.rem(peer, 4)], mlbuf.at[z], m_send, m_recv, "kv")
    w_copies = spread(lambda peer: wsend.at[lax.rem(peer, 4)], wbuf.at[z], w_send, w_recv, "kv")
    start_both(m_copies, w_copies)
    m_copies.arrive()
    ml = jnp.concatenate([mlbuf[j] for j in range(KV)], axis=0)
    shares = jnp.exp(ml - jnp.max(ml, axis=0, keepdims=True))
    grand = jnp.sum(shares * pltpu.roll(ml, half, 1), axis=0, keepdims=True)
    in_use = iota(ml.shape, 1) < quarter
    shares = jnp.where(in_use, shares / jnp.where(in_use[0:1], grand, 1.0), 0.0)
    columns = jnp.transpose(shares)
    w_copies.arrive()
    attended = columns[0:quarter, 0:1] * wbuf[0].astype(F32)
    for j in range(1, KV):
        attended = attended + columns[0:quarter, j : j + 1] * wbuf[j].astype(F32)
    ld_lam.wait()
    ld_hg.wait()
    lambdas = lam[0:1, 0:1]
    for g in range(1, heads):
        lambdas = jnp.where(
            lax.rem(iota((quarter, 1), 0), maps) // 2 == g, lam[0:1, g : g + 1], lambdas
        )
    diff = attended - lambdas * pltpu.roll(attended, quarter - 1, 0)
    normed = (
        diff
        * lax.rsqrt(jnp.mean(diff * diff, axis=1, keepdims=True) + EPS)
        * hg[...].astype(F32)
    ).astype(BF16)
    nbuf[mine] = normed
    spread(lambda peer: nbuf.at[mine], nbuf.at[mine], n_send, n_recv, "kv", (2, 1, KV - 1)).start().arrive()
    for c in range(4):
        lined_s[c * quarter : (c + 1) * quarter, :] = nbuf[c].astype(F32)
    outs = [lined_s[pl.ds(2 * g, rows, stride=maps), :] for g in range(heads)]
    heads_out = jnp.concatenate(outs, axis=1).astype(BF16)
    ld_wo.wait()
    dbuf[t] = dot(heads_out, wo[...])
    spread(lambda peer: dbuf.at[t], dbuf.at[t], d_send, d_recv, "tp").start().arrive()
    projected = dbuf[0]
    for j in range(1, TP):
        projected = projected + dbuf[j]
    mixed = (block + projected).astype(BF16).astype(F32)
    sqbuf[z] = to_lanes(jnp.sum(mixed * mixed, axis=1, keepdims=True))
    s_copies = spread(lambda peer: sqbuf.at[z], sqbuf.at[z], s_send, s_recv, "kv").start()
    ld_mg.wait()
    gain2 = jnp.concatenate([mg[k : k + 1, :] for k in range(width // LANES)], axis=1).astype(F32)
    scaled2 = (mixed * gain2).astype(BF16)
    ld_wu.wait()
    up = dot(scaled2, wu[...])
    owners = KV // 2
    owned = lax.rem(z, owners)
    share_width = up.shape[1] // owners
    for j in range(owners):
        us[j] = up[:, j * share_width : (j + 1) * share_width].astype(BF16)
    ur[z] = us[owned]
    u_copies = spread(lambda peer: us.at[lax.rem(peer, owners)], ur.at[z], u_send, u_recv, "kv").start()
    s_copies.arrive()
    square2 = sqbuf[0]
    for j in range(1, KV):
        square2 = square2 + sqbuf[j]
    inv2 = to_rows(lax.rsqrt(square2 / D + EPS), rows)
    u_copies.arrive()
    up_sum = ur[0].astype(F32)
    for j in range(1, KV):
        up_sum = up_sum + ur[j].astype(F32)
    act = jnp.maximum(inv2 * up_sum, 0.0)
    hbuf[owned] = (act * act).astype(BF16)
    near = [owners // 2]
    for d in range(owners // 2 - 1, 0, -1):
        near += [d, KV - d]
    spread(lambda peer: hbuf.at[owned], hbuf.at[owned], h_send, h_recv, "kv", near).start().arrive()
    hidden = jnp.concatenate([hbuf[j] for j in range(owners)], axis=1)
    ld_wd.wait()
    down = dot(hidden, wd[...])
    for k in range(width // LANES):
        fs[k] = down[:, k * LANES : (k + 1) * LANES]
    fr[t] = fs[t // per_tile]
    f_copies = spread(lambda peer: fs.at[peer // per_tile], fr.at[t], f_send, f_recv, "tp").start()
    for copies in started[:-1]:
        copies.sent()
    f_copies.arrive()
    y = fr[0]
    for j in range(1, TP):
        y = y + fr[j]
    for k in range(width // LANES):
        y = y + jnp.where(t // per_tile == k, mixed[:, k * LANES : (k + 1) * LANES], 0.0)
    result = y[:, 0:piece]
    for k in range(1, per_tile):
        result = jnp.where(lax.rem(t, per_tile) == k, y[:, k * piece : (k + 1) * piece], result)
    out_ref[...] = result.astype(out_ref.dtype)
    f_copies.sent()


def body(
    KV,
    TP,
    residual,
    cache_keys,
    cache_values,
    norm_gain,
    query_weight,
    key_weight,
    value_weight,
    head_lambda,
    head_gain,
    out_weight,
    mixer_gain,
    up_weight,
    down_weight,
):
    rows, piece = residual.shape
    positions, depth = cache_keys.shape[1], cache_keys.shape[3]
    width = out_weight.shape[1]
    qcols = query_weight.shape[1]
    lines = rows * qcols * 2 // LANES
    share = up_weight.shape[1] * 2 // KV
    any_spec = pl.BlockSpec(memory_space=pl.ANY)
    dma = pltpu.SemaphoreType.DMA
    keys = cache_keys.reshape(rows, positions, depth)
    values = cache_values.reshape(rows, positions, depth)
    args = (
        residual,
        keys,
        values,
        norm_gain.reshape(width // LANES, LANES),
        query_weight,
        key_weight,
        value_weight,
        head_lambda.reshape(1, -1),
        head_gain.reshape(1, -1),
        out_weight,
        mixer_gain.reshape(width // LANES, LANES),
        up_weight,
        down_weight,
    )
    kv_sems = [dma((KV - 1,))] * 2
    tp_sems = [dma((TP - 1,))] * 2
    return pl.pallas_call(
        functools.partial(kernel, KV, TP),
        out_shape=jax.ShapeDtypeStruct((rows, piece), residual.dtype),
        in_specs=[any_spec] * len(args),
        out_specs=pl.BlockSpec(memory_space=pltpu.VMEM),
        scratch_shapes=[
            pltpu.VMEM((rows, piece), BF16),
            pltpu.VMEM(keys.shape, BF16),
            pltpu.VMEM(values.shape, BF16),
            pltpu.VMEM((width // LANES, LANES), BF16),
            pltpu.VMEM((width, qcols + 2 * LANES), BF16),
            pltpu.VMEM((1, head_lambda.shape[0]), F32),
            pltpu.VMEM((1, head_gain.shape[0]), BF16),
            pltpu.VMEM(out_weight.shape, BF16),
            pltpu.VMEM((width // LANES, LANES), BF16),
            pltpu.VMEM(up_weight.shape, BF16),
            pltpu.VMEM(down_weight.shape, BF16),
            pltpu.VMEM((TP, rows, LANES), BF16),
            pltpu.VMEM((KV, rows, qcols), BF16),
            pltpu.VMEM((KV, 1, 3 * LANES), F32),
            pltpu.VMEM((KV, 1, 3 * LANES), F32),
            pltpu.VMEM((lines, LANES), F32),
            pltpu.VMEM((4, lines // 4, LANES), BF16),
            pltpu.VMEM((KV, lines // 4, LANES), BF16),
            pltpu.VMEM((4, 1, LANES), F32),
            pltpu.VMEM((KV, 1, LANES), F32),
            pltpu.VMEM((4, lines // 4, LANES), BF16),
            pltpu.VMEM((TP, rows, width), F32),
            pltpu.VMEM((KV, 1, LANES), F32),
            pltpu.VMEM((KV // 2, rows, share), BF16),
            pltpu.VMEM((KV, rows, share), BF16),
            pltpu.VMEM((KV // 2, rows, share), BF16),
            pltpu.VMEM((width // LANES, rows, LANES), F32),
            pltpu.VMEM((TP, rows, LANES), F32),
            pltpu.SemaphoreType.REGULAR((2,)),
            dma((13,)),
            *tp_sems,
            *kv_sems,
            *kv_sems,
            *kv_sems,
            *kv_sems,
            *kv_sems,
            *tp_sems,
            *kv_sems,
            *kv_sems,
            *kv_sems,
            *tp_sems,
        ],
        compiler_params=pltpu.CompilerParams(
            collective_id=0, has_side_effects=True, vmem_limit_bytes=64 * 1000 * 1000
        ),
        name="layer",
    )(*args)


def solution(mesh):
    in_specs = (
        P("grp", ("kv", "tp")),
        P("grp", "kv", "tp", None),
        P("grp", "kv", "tp", None),
        P("kv"),
        P("kv", "tp"),
        P("kv", "tp"),
        P("kv", "tp"),
        P("tp"),
        P(),
        P("tp", "kv"),
        P("kv"),
        P("kv", "tp"),
        P("tp", "kv"),
    )
    out_specs = P("grp", ("kv", "tp"))
    fn = functools.partial(body, mesh.shape["kv"], mesh.shape["tp"])
    return jax.shard_map(fn, mesh=mesh, in_specs=in_specs, out_specs=out_specs, check_vma=False)
```

```python
import functools

import jax
import jax.numpy as jnp
from jax import lax
from jax.experimental import pallas as pl
from jax.experimental.pallas import tpu as pltpu
from jax.sharding import PartitionSpec as P

EPS = 1e-06
MESH = pl.DeviceIdType.MESH
F32 = jnp.float32
BF16 = jnp.bfloat16
LANES = 128
LOW = -1e30


def far_first(n):
    def distance(k):
        odd = lax.rem(k, 2)
        return n // 2 + odd * ((k + 1) // 2) - (1 - odd) * (k // 2)

    return distance


def loop(n, step):
    def run(k, carry):
        step(k)
        return carry

    lax.fori_loop(0, n, run, 0)


def three(x):
    high = x.astype(BF16).astype(F32)
    mid = (x - high).astype(BF16).astype(F32)
    return high, mid, x - high - mid


def stacked(rows):
    at = iota((8, LANES), 0)
    out = jnp.zeros((8, LANES), F32)
    for k, row in enumerate(rows):
        out = jnp.where(at == k, row, out)
    return out


class Spread:
    def __init__(self, copy_to, distances, steps):
        self.copy_to, self.distances, self.steps = copy_to, distances, steps

    def each(self, act):
        if self.steps is None:
            for d in self.distances:
                act(self.copy_to(d))
        else:
            loop(self.steps, lambda k: act(self.copy_to(self.distances(k))))

    def start(self):
        self.each(lambda copy: copy.start())
        return self

    def arrive(self):
        self.each(lambda copy: copy.wait_recv())

    def sent(self):
        self.each(lambda copy: copy.wait_send())


def iota(shape, dim):
    return lax.broadcasted_iota(jnp.int32, shape, dim)


def dot(a, b):
    return jnp.dot(a, b, preferred_element_type=F32)


def to_lanes(column):
    wide = jnp.broadcast_to(column, (column.shape[0], LANES))
    diagonal = iota(wide.shape, 0) == iota(wide.shape, 1)
    return jnp.sum(jnp.where(diagonal, wide, 0.0), axis=0, keepdims=True)


def to_rows(row, rows):
    wide = jnp.broadcast_to(row, (rows, LANES))
    diagonal = iota(wide.shape, 0) == iota(wide.shape, 1)
    return jnp.sum(jnp.where(diagonal, wide, 0.0), axis=1, keepdims=True)


def kernel(
    KV,
    TP,
    res_h,
    keys_h,
    values_h,
    ng_h,
    wq_h,
    wk_h,
    wv_h,
    lam_h,
    hg_h,
    wo_h,
    mg_h,
    wu_h,
    wd_h,
    out_ref,
    res,
    keys,
    values,
    ng,
    wp,
    lam,
    hg,
    wo,
    mg,
    wu,
    wd,
    abuf,
    qsend,
    qbuf,
    lined_s,
    wsend,
    wbuf,
    nbuf,
    dbuf,
    sqbuf,
    us,
    ur,
    hbuf,
    fs,
    fr,
    ring_sem,
    load_sem,
    a_send,
    a_recv,
    q_send,
    q_recv,
    w_send,
    w_recv,
    n_send,
    n_recv,
    d_send,
    d_recv,
    s_send,
    s_recv,
    u_send,
    u_recv,
    h_send,
    h_recv,
    f_send,
    f_recv,
):
    z = lax.axis_index("kv")
    t = lax.axis_index("tp")
    rows = res_h.shape[0]
    piece = res_h.shape[1]
    per_tile = LANES // piece
    width = wo.shape[1]
    D = KV * width
    qcols = wq_h.shape[1]
    heads = qcols // LANES
    half = LANES // 2
    maps = heads * 2
    lines = rows * maps

    def load(src, dst, k):
        copy = pltpu.make_async_copy(src, dst, load_sem.at[k])
        copy.start()
        return copy

    ld_res = load(res_h, res, 0)
    barrier = pltpu.get_barrier_semaphore()
    def greet(k):
        peer = lax.rem(t + k + 1, TP)
        pl.semaphore_signal(barrier, inc=1, device_id={"tp": peer}, device_id_type=MESH)

    loop(TP - 1, greet)

    def both_ways(sem, d):
        for u in (d, KV - d):
            peer = lax.rem(z + u, KV)
            pl.semaphore_signal(sem, inc=1, device_id={"kv": peer}, device_id_type=MESH)

    both_ways(barrier, 1)
    both_ways(barrier, 2)
    ld_ng = load(ng_h, ng, 1)
    ld_wq = load(wq_h, wp.at[:, 0:qcols], 2)
    ld_wk = load(wk_h, wp.at[:, qcols : qcols + LANES], 3)
    ld_wv = load(wv_h, wp.at[:, qcols + LANES : qcols + 2 * LANES], 4)

    started = []

    def spread(src_of, dst, ssem, rsem, axis, distances=None):
        me, n = (z, KV) if axis == "kv" else (t, TP)

        def copy_to(d):
            peer = lax.rem(me + d, n)
            return pltpu.make_async_remote_copy(
                src_ref=src_of(peer),
                dst_ref=dst,
                send_sem=ssem.at[d - 1],
                recv_sem=rsem.at[d - 1],
                device_id={axis: peer},
                device_id_type=MESH,
            )

        if distances is None:
            out = Spread(copy_to, far_first(n), n - 1)
        else:
            out = Spread(copy_to, distances, None)
        started.append(out)
        return out

    ld_res.wait()
    own_piece = res[...].astype(F32)
    tiled = jnp.concatenate([own_piece] * per_tile, axis=1)
    at = iota(tiled.shape, 1) // piece == lax.rem(t, per_tile)
    abuf[t] = jnp.where(at, tiled, 0.0).astype(BF16)
    pl.semaphore_wait(barrier, TP - 1 + 4)
    a_copies = spread(lambda peer: abuf.at[t], abuf.at[t], a_send, a_recv, "tp").start()
    both_ways(ring_sem.at[0], 2)
    pl.semaphore_wait(ring_sem.at[0], 2)
    both_ways(ring_sem.at[1], 4)
    a_copies.arrive()
    block = jnp.concatenate(
        [
            sum(abuf[k * per_tile + j].astype(F32) for j in range(per_tile))
            for k in range(TP // per_tile)
        ],
        axis=1,
    )
    ld_ng.wait()
    gain = jnp.concatenate([ng[k : k + 1, :] for k in range(width // LANES)], axis=1).astype(F32)
    scaled = (block * gain).astype(BF16)
    ld_wq.wait()
    ld_wk.wait()
    ld_wv.wait()
    proj = dot(scaled, wp[...])
    square = to_lanes(jnp.sum(block * block, axis=1, keepdims=True))
    extra = stacked((square, square, *three(square)))
    at = iota((8, LANES), 0)
    for j in range(KV):
        for g in range(heads):
            qsend[j, g * rows : (g + 1) * rows, :] = proj[:, g * LANES : (g + 1) * LANES].astype(BF16)
        key_row = proj[j : j + 1, qcols : qcols + LANES]
        value_row = proj[j : j + 1, qcols + LANES :]
        last = jnp.where(at == 0, key_row, jnp.where(at == 1, value_row, extra))
        qsend[j, heads * rows :, :] = last.astype(BF16)
    qbuf[z] = qsend[z]
    pl.semaphore_wait(ring_sem.at[1], 2)
    q_copies = spread(lambda peer: qsend.at[peer], qbuf.at[z], q_send, q_recv, "kv").start()
    ld_keys = load(keys_h, keys, 5)
    ld_values = load(values_h, values, 6)
    ld_lam = load(lam_h, lam, 7)
    ld_hg = load(hg_h, hg, 8)
    ld_wo = load(wo_h, wo, 9)
    ld_mg = load(mg_h, mg, 10)
    ld_wu = load(wu_h, wu, 11)
    ld_wd = load(wd_h, wd, 12)
    q_copies.arrive()
    q_sum = qbuf[0].astype(F32)
    for j in range(1, KV):
        q_sum = q_sum + qbuf[j].astype(F32)
    r_sum = q_sum[heads * rows :]
    inv_lanes = lax.rsqrt((r_sum[2:3] + r_sum[3:4] + r_sum[4:5]) / D + EPS)
    inv_own = jnp.sum(
        jnp.where(iota(inv_lanes.shape, 1) == z, inv_lanes, 0.0), axis=1, keepdims=True
    )
    new_key = (inv_own * r_sum[0:1]).astype(BF16).astype(F32)
    new_value = (inv_own * r_sum[1:2]).astype(BF16).astype(F32)
    inv_rows = to_rows(inv_lanes, rows)

    lane = iota((rows, LANES), 1)
    for g in range(heads):
        head = (inv_rows * q_sum[g * rows : (g + 1) * rows]).astype(BF16)
        head = head.astype(F32) * (1.0 / half**0.5)
        for c in range(2):
            lined_s[pl.ds(2 * g + c, rows, stride=maps), :] = jnp.where(lane // half == c, head, 0.0)
    lined = lined_s[...]

    ld_keys.wait()
    ld_values.wait()
    tops, totals, sums = [], [], []
    for p in range(lines // 8):
        seqs = 8 // maps
        qp = lined[8 * p : 8 * p + 8, :].astype(BF16)
        scores = None
        for k in range(seqs):
            part = lax.dot_general(
                qp, keys[seqs * p + k], (((1,), (1,)), ((), ())), preferred_element_type=F32
            )
            if scores is None:
                scores = part
            else:
                scores = jnp.where(iota(part.shape, 0) // maps == k, part, scores)
        top = jnp.max(scores, axis=1, keepdims=True)
        expo = jnp.exp(scores - top)
        total = jnp.sum(expo, axis=1, keepdims=True)
        probs = expo.astype(BF16)
        weighted = None
        for k in range(seqs):
            part = dot(probs, values[seqs * p + k])
            if weighted is None:
                weighted = part
            else:
                weighted = jnp.where(iota(part.shape, 0) // maps == k, part, weighted)
        tops.append(top)
        totals.append(total)
        sums.append(weighted)
    top = jnp.concatenate(tops, axis=0)
    total = jnp.concatenate(totals, axis=0)
    weighted = jnp.concatenate(sums, axis=0)
    own = jnp.sum(lined * new_key, axis=1, keepdims=True)
    own = jnp.where(iota(own.shape, 0) // maps == z, own, LOW)
    new_top = jnp.maximum(top, own)
    old_part = jnp.exp(top - new_top)
    own_part = jnp.exp(own - new_top)
    total = total * old_part + own_part
    weighted = weighted * old_part + own_part * new_value
    quarter = lines // 4
    mine = lax.rem(z, 4)
    for c in range(4):
        at = slice(c * quarter, (c + 1) * quarter)
        wsend[c, 0:quarter, :] = weighted[at].astype(BF16)
        both = stacked((*three(to_lanes(new_top[at])), *three(to_lanes(total[at]))))
        wsend[c, quarter:, :] = both.astype(BF16)
    wbuf[z] = wsend[mine]
    w_copies = spread(lambda peer: wsend.at[lax.rem(peer, 4)], wbuf.at[z], w_send, w_recv, "kv").start()
    w_copies.arrive()
    tails = [wbuf[j, quarter:, :].astype(F32) for j in range(KV)]
    ml = jnp.concatenate([x[0:1] + x[1:2] + x[2:3] for x in tails], axis=0)
    totals = jnp.concatenate([x[3:4] + x[4:5] + x[5:6] for x in tails], axis=0)
    shares = jnp.exp(ml - jnp.max(ml, axis=0, keepdims=True))
    grand = jnp.sum(shares * totals, axis=0, keepdims=True)
    in_use = iota(ml.shape, 1) < quarter
    shares = jnp.where(in_use, shares / jnp.where(in_use[0:1], grand, 1.0), 0.0)
    columns = jnp.transpose(shares)
    attended = columns[0:quarter, 0:1] * wbuf[0, 0:quarter, :].astype(F32)
    for j in range(1, KV):
        attended = attended + columns[0:quarter, j : j + 1] * wbuf[j, 0:quarter, :].astype(F32)
    ld_lam.wait()
    ld_hg.wait()
    lambdas = lam[0:1, 0:1]
    for g in range(1, heads):
        lambdas = jnp.where(
            lax.rem(iota((quarter, 1), 0), maps) // 2 == g, lam[0:1, g : g + 1], lambdas
        )
    diff = attended - lambdas * pltpu.roll(attended, quarter - 1, 0)
    normed = (
        diff
        * lax.rsqrt(jnp.mean(diff * diff, axis=1, keepdims=True) + EPS)
        * hg[...].astype(F32)
    ).astype(BF16)
    nbuf[mine] = normed
    spread(lambda peer: nbuf.at[mine], nbuf.at[mine], n_send, n_recv, "kv", (2, 1, KV - 1)).start().arrive()
    for c in range(4):
        lined_s[c * quarter : (c + 1) * quarter, :] = nbuf[c].astype(F32)
    outs = [lined_s[pl.ds(2 * g, rows, stride=maps), :] for g in range(heads)]
    heads_out = jnp.concatenate(outs, axis=1).astype(BF16)
    ld_wo.wait()
    dbuf[t] = dot(heads_out, wo[...])
    spread(lambda peer: dbuf.at[t], dbuf.at[t], d_send, d_recv, "tp").start().arrive()
    projected = dbuf[0]
    for j in range(1, TP):
        projected = projected + dbuf[j]
    mixed = (block + projected).astype(BF16).astype(F32)
    sqbuf[z] = to_lanes(jnp.sum(mixed * mixed, axis=1, keepdims=True))
    ld_mg.wait()
    gain2 = jnp.concatenate([mg[k : k + 1, :] for k in range(width // LANES)], axis=1).astype(F32)
    scaled2 = (mixed * gain2).astype(BF16)
    ld_wu.wait()
    up = dot(scaled2, wu[...])
    owners = KV // 2
    owned = lax.rem(z, owners)
    share_width = up.shape[1] // owners
    for j in range(owners):
        us[j] = up[:, j * share_width : (j + 1) * share_width].astype(BF16)
    ur[z] = us[owned]
    u_copies = spread(lambda peer: us.at[lax.rem(peer, owners)], ur.at[z], u_send, u_recv, "kv").start()
    s_copies = spread(lambda peer: sqbuf.at[z], sqbuf.at[z], s_send, s_recv, "kv").start()
    u_copies.arrive()
    up_sum = ur[0].astype(F32)
    for j in range(1, KV):
        up_sum = up_sum + ur[j].astype(F32)
    act = jnp.maximum(up_sum, 0.0)
    hbuf[owned] = (act * act).astype(BF16)
    near = [owners // 2]
    for d in range(owners // 2 - 1, 0, -1):
        near += [d, KV - d]
    spread(lambda peer: hbuf.at[owned], hbuf.at[owned], h_send, h_recv, "kv", near).start().arrive()
    hidden = jnp.concatenate([hbuf[j] for j in range(owners)], axis=1)
    ld_wd.wait()
    down = dot(hidden, wd[...])
    for k in range(width // LANES):
        fs[k] = down[:, k * LANES : (k + 1) * LANES]
    fr[t] = fs[t // per_tile]
    f_copies = spread(lambda peer: fs.at[peer // per_tile], fr.at[t], f_send, f_recv, "tp").start()
    for copies in started[:-1]:
        copies.sent()
    s_copies.arrive()
    square2 = sqbuf[0]
    for j in range(1, KV):
        square2 = square2 + sqbuf[j]
    inv2 = to_rows(1.0 / (square2 / D + EPS), rows)
    f_copies.arrive()
    y = fr[0]
    for j in range(1, TP):
        y = y + fr[j]
    y = inv2 * y
    for k in range(width // LANES):
        y = y + jnp.where(t // per_tile == k, mixed[:, k * LANES : (k + 1) * LANES], 0.0)
    result = y[:, 0:piece]
    for k in range(1, per_tile):
        result = jnp.where(lax.rem(t, per_tile) == k, y[:, k * piece : (k + 1) * piece], result)
    out_ref[...] = result.astype(out_ref.dtype)
    f_copies.sent()


def body(
    KV,
    TP,
    residual,
    cache_keys,
    cache_values,
    norm_gain,
    query_weight,
    key_weight,
    value_weight,
    head_lambda,
    head_gain,
    out_weight,
    mixer_gain,
    up_weight,
    down_weight,
):
    rows, piece = residual.shape
    positions, depth = cache_keys.shape[1], cache_keys.shape[3]
    width = out_weight.shape[1]
    qcols = query_weight.shape[1]
    lines = rows * qcols * 2 // LANES
    share = up_weight.shape[1] * 2 // KV
    any_spec = pl.BlockSpec(memory_space=pl.ANY)
    dma = pltpu.SemaphoreType.DMA
    keys = cache_keys.reshape(rows, positions, depth)
    values = cache_values.reshape(rows, positions, depth)
    args = (
        residual,
        keys,
        values,
        norm_gain.reshape(width // LANES, LANES),
        query_weight,
        key_weight,
        value_weight,
        head_lambda.reshape(1, -1),
        head_gain.reshape(1, -1),
        out_weight,
        mixer_gain.reshape(width // LANES, LANES),
        up_weight,
        down_weight,
    )
    kv_sems = [dma((KV - 1,))] * 2
    tp_sems = [dma((TP - 1,))] * 2
    return pl.pallas_call(
        functools.partial(kernel, KV, TP),
        out_shape=jax.ShapeDtypeStruct((rows, piece), residual.dtype),
        in_specs=[any_spec] * len(args),
        out_specs=pl.BlockSpec(memory_space=pltpu.VMEM),
        scratch_shapes=[
            pltpu.VMEM((rows, piece), BF16),
            pltpu.VMEM(keys.shape, BF16),
            pltpu.VMEM(values.shape, BF16),
            pltpu.VMEM((width // LANES, LANES), BF16),
            pltpu.VMEM((width, qcols + 2 * LANES), BF16),
            pltpu.VMEM((1, head_lambda.shape[0]), F32),
            pltpu.VMEM((1, head_gain.shape[0]), BF16),
            pltpu.VMEM(out_weight.shape, BF16),
            pltpu.VMEM((width // LANES, LANES), BF16),
            pltpu.VMEM(up_weight.shape, BF16),
            pltpu.VMEM(down_weight.shape, BF16),
            pltpu.VMEM((TP, rows, LANES), BF16),
            pltpu.VMEM((KV, rows * qcols // LANES + 8, LANES), BF16),
            pltpu.VMEM((KV, rows * qcols // LANES + 8, LANES), BF16),
            pltpu.VMEM((lines, LANES), F32),
            pltpu.VMEM((4, lines // 4 + 8, LANES), BF16),
            pltpu.VMEM((KV, lines // 4 + 8, LANES), BF16),
            pltpu.VMEM((4, lines // 4, LANES), BF16),
            pltpu.VMEM((TP, rows, width), F32),
            pltpu.VMEM((KV, 1, LANES), F32),
            pltpu.VMEM((KV // 2, rows, share), BF16),
            pltpu.VMEM((KV, rows, share), BF16),
            pltpu.VMEM((KV // 2, rows, share), BF16),
            pltpu.VMEM((width // LANES, rows, LANES), F32),
            pltpu.VMEM((TP, rows, LANES), F32),
            pltpu.SemaphoreType.REGULAR((2,)),
            dma((13,)),
            *tp_sems,
            *kv_sems,
            *kv_sems,
            *kv_sems,
            *tp_sems,
            *kv_sems,
            *kv_sems,
            *kv_sems,
            *tp_sems,
        ],
        compiler_params=pltpu.CompilerParams(
            collective_id=0, has_side_effects=True, vmem_limit_bytes=64 * 1000 * 1000
        ),
        name="layer",
    )(*args)


def solution(mesh):
    in_specs = (
        P("grp", ("kv", "tp")),
        P("grp", "kv", "tp", None),
        P("grp", "kv", "tp", None),
        P("kv"),
        P("kv", "tp"),
        P("kv", "tp"),
        P("kv", "tp"),
        P("tp"),
        P(),
        P("tp", "kv"),
        P("kv"),
        P("kv", "tp"),
        P("tp", "kv"),
    )
    out_specs = P("grp", ("kv", "tp"))
    fn = functools.partial(body, mesh.shape["kv"], mesh.shape["tp"])
    return jax.shard_map(fn, mesh=mesh, in_specs=in_specs, out_specs=out_specs, check_vma=False)
```

```python
import functools

import jax
import jax.numpy as jnp
from jax import lax
from jax.experimental import pallas as pl
from jax.experimental.pallas import tpu as pltpu
from jax.sharding import PartitionSpec as P

EPS = 1e-06
MESH = pl.DeviceIdType.MESH
F32 = jnp.float32
BF16 = jnp.bfloat16
LANES = 128
LOW = -1e30


def far_first(n):
    def distance(k):
        odd = lax.rem(k, 2)
        return n // 2 + odd * ((k + 1) // 2) - (1 - odd) * (k // 2)

    return distance


def loop(n, step):
    def run(k, carry):
        step(k)
        return carry

    lax.fori_loop(0, n, run, 0)


def three(x):
    high = x.astype(BF16).astype(F32)
    mid = (x - high).astype(BF16).astype(F32)
    return high, mid, x - high - mid


def stacked(rows):
    at = iota((8, LANES), 0)
    out = jnp.zeros((8, LANES), F32)
    for k, row in enumerate(rows):
        out = jnp.where(at == k, row, out)
    return out


class Spread:
    def __init__(self, copy, copy_to, distances, steps, peer, slots):
        self.copy_to, self.distances, self.steps = copy_to, distances, steps
        self.whole = copy(slots, slots, peer)

    def start(self):
        if self.steps is None:
            for d in self.distances:
                self.copy_to(d).start()
        else:
            loop(self.steps, lambda k: self.copy_to(self.distances(k)).start())
        return self

    def arrive(self):
        self.whole.wait_recv()
        self.whole.wait_send()


def iota(shape, dim):
    return lax.broadcasted_iota(jnp.int32, shape, dim)


def dot(a, b):
    return jnp.dot(a, b, preferred_element_type=F32)


def to_lanes(column):
    wide = jnp.broadcast_to(column, (column.shape[0], LANES))
    diagonal = iota(wide.shape, 0) == iota(wide.shape, 1)
    return jnp.sum(jnp.where(diagonal, wide, 0.0), axis=0, keepdims=True)


def to_rows(row, rows):
    wide = jnp.broadcast_to(row, (rows, LANES))
    diagonal = iota(wide.shape, 0) == iota(wide.shape, 1)
    return jnp.sum(jnp.where(diagonal, wide, 0.0), axis=1, keepdims=True)


def kernel(
    KV,
    TP,
    res_h,
    keys_h,
    values_h,
    ng_h,
    wq_h,
    wk_h,
    wv_h,
    lam_h,
    hg_h,
    wo_h,
    mg_h,
    wu_h,
    wd_h,
    out_ref,
    res,
    keys,
    values,
    ng,
    wp,
    lam,
    hg,
    wo,
    mg,
    wu,
    wd,
    abuf,
    qsend,
    qbuf,
    lined_s,
    wsend,
    wbuf,
    nbuf,
    dbuf,
    sqbuf,
    us,
    ur,
    hbuf,
    fs,
    fr,
    ring_sem,
    load_sem,
    send_sem,
    recv_sem,
):
    z = lax.axis_index("kv")
    t = lax.axis_index("tp")
    rows = res_h.shape[0]
    piece = res_h.shape[1]
    per_tile = LANES // piece
    width = wo.shape[1]
    D = KV * width
    qcols = wq_h.shape[1]
    heads = qcols // LANES
    half = LANES // 2
    maps = heads * 2
    lines = rows * maps

    def load(src, dst, k):
        copy = pltpu.make_async_copy(src, dst, load_sem.at[k])
        copy.start()
        return copy

    ld_res = load(res_h, res, 0)
    barrier = pltpu.get_barrier_semaphore()
    def greet(k):
        peer = lax.rem(t + k + 1, TP)
        pl.semaphore_signal(barrier, inc=1, device_id={"tp": peer}, device_id_type=MESH)

    loop(TP - 1, greet)

    def both_ways(sem, d):
        for u in (d, KV - d):
            peer = lax.rem(z + u, KV)
            pl.semaphore_signal(sem, inc=1, device_id={"kv": peer}, device_id_type=MESH)

    both_ways(barrier, 1)
    both_ways(barrier, 2)
    ld_ng = load(ng_h, ng, 1)
    ld_wq = load(wq_h, wp.at[:, 0:qcols], 2)
    ld_wk = load(wk_h, wp.at[:, qcols : qcols + LANES], 3)
    ld_wv = load(wv_h, wp.at[:, qcols + LANES : qcols + 2 * LANES], 4)

    def spread(src_of, dst, buf, ssem, rsem, axis, distances=None):
        me, n = (z, KV) if axis == "kv" else (t, TP)
        steps = n - 1 if distances is None else None
        count = n - 1 if distances is None else len(distances)

        def copy(src, dst, peer):
            return pltpu.make_async_remote_copy(
                src_ref=src,
                dst_ref=dst,
                send_sem=ssem,
                recv_sem=rsem,
                device_id={axis: peer},
                device_id_type=MESH,
            )

        def copy_to(d):
            peer = lax.rem(me + d, n)
            return copy(src_of(peer), dst, peer)

        order = far_first(n) if distances is None else distances
        slots = buf.at[pl.ds(0, count)]
        return Spread(copy, copy_to, order, steps, lax.rem(me + 1, n), slots)

    ld_res.wait()
    own_piece = res[...].astype(F32)
    tiled = jnp.concatenate([own_piece] * per_tile, axis=1)
    at = iota(tiled.shape, 1) // piece == lax.rem(t, per_tile)
    abuf[t] = jnp.where(at, tiled, 0.0).astype(BF16)
    pl.semaphore_wait(barrier, TP - 1 + 4)
    a_copies = spread(lambda peer: abuf.at[t], abuf.at[t], abuf, send_sem.at[0], recv_sem.at[0], "tp").start()
    both_ways(ring_sem.at[0], 2)
    pl.semaphore_wait(ring_sem.at[0], 2)
    both_ways(ring_sem.at[1], 4)
    a_copies.arrive()
    block = jnp.concatenate(
        [
            sum(abuf[k * per_tile + j].astype(F32) for j in range(per_tile))
            for k in range(TP // per_tile)
        ],
        axis=1,
    )
    ld_ng.wait()
    gain = jnp.concatenate([ng[k : k + 1, :] for k in range(width // LANES)], axis=1).astype(F32)
    scaled = (block * gain).astype(BF16)
    ld_wq.wait()
    ld_wk.wait()
    ld_wv.wait()
    proj = dot(scaled, wp[...])
    square = to_lanes(jnp.sum(block * block, axis=1, keepdims=True))
    extra = stacked((square, square, *three(square)))
    at = iota((8, LANES), 0)
    for j in range(KV):
        for g in range(heads):
            qsend[j, g * rows : (g + 1) * rows, :] = proj[:, g * LANES : (g + 1) * LANES].astype(BF16)
        key_row = proj[j : j + 1, qcols : qcols + LANES]
        value_row = proj[j : j + 1, qcols + LANES :]
        last = jnp.where(at == 0, key_row, jnp.where(at == 1, value_row, extra))
        qsend[j, heads * rows :, :] = last.astype(BF16)
    qbuf[z] = qsend[z]
    pl.semaphore_wait(ring_sem.at[1], 2)
    q_copies = spread(lambda peer: qsend.at[peer], qbuf.at[z], qbuf, send_sem.at[0], recv_sem.at[1], "kv").start()
    ld_keys = load(keys_h, keys, 0)
    ld_values = load(values_h, values, 1)
    ld_lam = load(lam_h, lam, 2)
    ld_hg = load(hg_h, hg, 3)
    ld_wo = load(wo_h, wo, 4)
    ld_mg = load(mg_h, mg, 5)
    ld_wu = load(wu_h, wu, 6)
    ld_wd = load(wd_h, wd, 7)
    q_copies.arrive()
    q_sum = qbuf[0].astype(F32)
    for j in range(1, KV):
        q_sum = q_sum + qbuf[j].astype(F32)
    r_sum = q_sum[heads * rows :]
    inv_lanes = lax.rsqrt((r_sum[2:3] + r_sum[3:4] + r_sum[4:5]) / D + EPS)
    inv_own = jnp.sum(
        jnp.where(iota(inv_lanes.shape, 1) == z, inv_lanes, 0.0), axis=1, keepdims=True
    )
    new_key = (inv_own * r_sum[0:1]).astype(BF16).astype(F32)
    new_value = (inv_own * r_sum[1:2]).astype(BF16).astype(F32)
    inv_rows = to_rows(inv_lanes, rows)

    lane = iota((rows, LANES), 1)
    for g in range(heads):
        head = (inv_rows * q_sum[g * rows : (g + 1) * rows]).astype(BF16)
        head = head.astype(F32) * (1.0 / half**0.5)
        for c in range(2):
            lined_s[pl.ds(2 * g + c, rows, stride=maps), :] = jnp.where(lane // half == c, head, 0.0)
    lined = lined_s[...]

    ld_keys.wait()
    ld_values.wait()
    tops, totals, sums = [], [], []
    for p in range(lines // 8):
        seqs = 8 // maps
        qp = lined[8 * p : 8 * p + 8, :].astype(BF16)
        scores = None
        for k in range(seqs):
            part = lax.dot_general(
                qp, keys[seqs * p + k], (((1,), (1,)), ((), ())), preferred_element_type=F32
            )
            if scores is None:
                scores = part
            else:
                scores = jnp.where(iota(part.shape, 0) // maps == k, part, scores)
        top = jnp.max(scores, axis=1, keepdims=True)
        expo = jnp.exp(scores - top)
        total = jnp.sum(expo, axis=1, keepdims=True)
        probs = expo.astype(BF16)
        weighted = None
        for k in range(seqs):
            part = dot(probs, values[seqs * p + k])
            if weighted is None:
                weighted = part
            else:
                weighted = jnp.where(iota(part.shape, 0) // maps == k, part, weighted)
        tops.append(top)
        totals.append(total)
        sums.append(weighted)
    top = jnp.concatenate(tops, axis=0)
    total = jnp.concatenate(totals, axis=0)
    weighted = jnp.concatenate(sums, axis=0)
    own = jnp.sum(lined * new_key, axis=1, keepdims=True)
    own = jnp.where(iota(own.shape, 0) // maps == z, own, LOW)
    new_top = jnp.maximum(top, own)
    old_part = jnp.exp(top - new_top)
    own_part = jnp.exp(own - new_top)
    total = total * old_part + own_part
    weighted = weighted * old_part + own_part * new_value
    quarter = lines // 4
    mine = lax.rem(z, 4)
    for c in range(4):
        at = slice(c * quarter, (c + 1) * quarter)
        wsend[c, 0:quarter, :] = weighted[at].astype(BF16)
        both = stacked((*three(to_lanes(new_top[at])), *three(to_lanes(total[at]))))
        wsend[c, quarter:, :] = both.astype(BF16)
    wbuf[z] = wsend[mine]
    w_copies = spread(lambda peer: wsend.at[lax.rem(peer, 4)], wbuf.at[z], wbuf, send_sem.at[0], recv_sem.at[2], "kv").start()
    w_copies.arrive()
    tails = [wbuf[j, quarter:, :].astype(F32) for j in range(KV)]
    ml = jnp.concatenate([x[0:1] + x[1:2] + x[2:3] for x in tails], axis=0)
    totals = jnp.concatenate([x[3:4] + x[4:5] + x[5:6] for x in tails], axis=0)
    shares = jnp.exp(ml - jnp.max(ml, axis=0, keepdims=True))
    grand = jnp.sum(shares * totals, axis=0, keepdims=True)
    in_use = iota(ml.shape, 1) < quarter
    shares = jnp.where(in_use, shares / jnp.where(in_use[0:1], grand, 1.0), 0.0)
    columns = jnp.transpose(shares)
    attended = columns[0:quarter, 0:1] * wbuf[0, 0:quarter, :].astype(F32)
    for j in range(1, KV):
        attended = attended + columns[0:quarter, j : j + 1] * wbuf[j, 0:quarter, :].astype(F32)
    ld_lam.wait()
    ld_hg.wait()
    lambdas = lam[0:1, 0:1]
    for g in range(1, heads):
        lambdas = jnp.where(
            lax.rem(iota((quarter, 1), 0), maps) // 2 == g, lam[0:1, g : g + 1], lambdas
        )
    diff = attended - lambdas * pltpu.roll(attended, quarter - 1, 0)
    normed = (
        diff
        * lax.rsqrt(jnp.mean(diff * diff, axis=1, keepdims=True) + EPS)
        * hg[...].astype(F32)
    ).astype(BF16)
    nbuf[mine] = normed
    spread(lambda peer: nbuf.at[mine], nbuf.at[mine], nbuf, send_sem.at[0], recv_sem.at[3], "kv", (2, 1, KV - 1)).start().arrive()
    for c in range(4):
        lined_s[c * quarter : (c + 1) * quarter, :] = nbuf[c].astype(F32)
    outs = [lined_s[pl.ds(2 * g, rows, stride=maps), :] for g in range(heads)]
    heads_out = jnp.concatenate(outs, axis=1).astype(BF16)
    ld_wo.wait()
    dbuf[t] = dot(heads_out, wo[...])
    spread(lambda peer: dbuf.at[t], dbuf.at[t], dbuf, send_sem.at[0], recv_sem.at[4], "tp").start().arrive()
    projected = dbuf[0]
    for j in range(1, TP):
        projected = projected + dbuf[j]
    mixed = (block + projected).astype(BF16).astype(F32)
    sqbuf[z] = to_lanes(jnp.sum(mixed * mixed, axis=1, keepdims=True))
    ld_mg.wait()
    gain2 = jnp.concatenate([mg[k : k + 1, :] for k in range(width // LANES)], axis=1).astype(F32)
    scaled2 = (mixed * gain2).astype(BF16)
    ld_wu.wait()
    up = dot(scaled2, wu[...])
    owners = KV // 2
    owned = lax.rem(z, owners)
    share_width = up.shape[1] // owners
    for j in range(owners):
        us[j] = up[:, j * share_width : (j + 1) * share_width].astype(BF16)
    ur[z] = us[owned]
    u_copies = spread(lambda peer: us.at[lax.rem(peer, owners)], ur.at[z], ur, send_sem.at[0], recv_sem.at[5], "kv").start()
    s_copies = spread(lambda peer: sqbuf.at[z], sqbuf.at[z], sqbuf, send_sem.at[1], recv_sem.at[6], "kv").start()
    u_copies.arrive()
    up_sum = ur[0].astype(F32)
    for j in range(1, KV):
        up_sum = up_sum + ur[j].astype(F32)
    act = jnp.maximum(up_sum, 0.0)
    hbuf[owned] = (act * act).astype(BF16)
    near = [owners // 2]
    for d in range(owners // 2 - 1, 0, -1):
        near += [d, KV - d]
    spread(lambda peer: hbuf.at[owned], hbuf.at[owned], hbuf, send_sem.at[0], recv_sem.at[7], "kv", near).start().arrive()
    hidden = jnp.concatenate([hbuf[j] for j in range(owners)], axis=1)
    ld_wd.wait()
    down = dot(hidden, wd[...])
    for k in range(width // LANES):
        fs[k] = down[:, k * LANES : (k + 1) * LANES]
    fr[t] = fs[t // per_tile]
    f_copies = spread(lambda peer: fs.at[peer // per_tile], fr.at[t], fr, send_sem.at[0], recv_sem.at[8], "tp").start()
    s_copies.arrive()
    square2 = sqbuf[0]
    for j in range(1, KV):
        square2 = square2 + sqbuf[j]
    inv2 = to_rows(1.0 / (square2 / D + EPS), rows)
    f_copies.arrive()
    y = fr[0]
    for j in range(1, TP):
        y = y + fr[j]
    y = inv2 * y
    for k in range(width // LANES):
        y = y + jnp.where(t // per_tile == k, mixed[:, k * LANES : (k + 1) * LANES], 0.0)
    result = y[:, 0:piece]
    for k in range(1, per_tile):
        result = jnp.where(lax.rem(t, per_tile) == k, y[:, k * piece : (k + 1) * piece], result)
    out_ref[...] = result.astype(out_ref.dtype)


def body(
    KV,
    TP,
    residual,
    cache_keys,
    cache_values,
    norm_gain,
    query_weight,
    key_weight,
    value_weight,
    head_lambda,
    head_gain,
    out_weight,
    mixer_gain,
    up_weight,
    down_weight,
):
    rows, piece = residual.shape
    positions, depth = cache_keys.shape[1], cache_keys.shape[3]
    width = out_weight.shape[1]
    qcols = query_weight.shape[1]
    lines = rows * qcols * 2 // LANES
    share = up_weight.shape[1] * 2 // KV
    any_spec = pl.BlockSpec(memory_space=pl.ANY)
    dma = pltpu.SemaphoreType.DMA
    keys = cache_keys.reshape(rows, positions, depth)
    values = cache_values.reshape(rows, positions, depth)
    args = (
        residual,
        keys,
        values,
        norm_gain.reshape(width // LANES, LANES),
        query_weight,
        key_weight,
        value_weight,
        head_lambda.reshape(1, -1),
        head_gain.reshape(1, -1),
        out_weight,
        mixer_gain.reshape(width // LANES, LANES),
        up_weight,
        down_weight,
    )
    return pl.pallas_call(
        functools.partial(kernel, KV, TP),
        out_shape=jax.ShapeDtypeStruct((rows, piece), residual.dtype),
        in_specs=[any_spec] * len(args),
        out_specs=pl.BlockSpec(memory_space=pltpu.VMEM),
        scratch_shapes=[
            pltpu.VMEM((rows, piece), BF16),
            pltpu.VMEM(keys.shape, BF16),
            pltpu.VMEM(values.shape, BF16),
            pltpu.VMEM((width // LANES, LANES), BF16),
            pltpu.VMEM((width, qcols + 2 * LANES), BF16),
            pltpu.VMEM((1, head_lambda.shape[0]), F32),
            pltpu.VMEM((1, head_gain.shape[0]), BF16),
            pltpu.VMEM(out_weight.shape, BF16),
            pltpu.VMEM((width // LANES, LANES), BF16),
            pltpu.VMEM(up_weight.shape, BF16),
            pltpu.VMEM(down_weight.shape, BF16),
            pltpu.VMEM((TP, rows, LANES), BF16),
            pltpu.VMEM((KV, rows * qcols // LANES + 8, LANES), BF16),
            pltpu.VMEM((KV, rows * qcols // LANES + 8, LANES), BF16),
            pltpu.VMEM((lines, LANES), F32),
            pltpu.VMEM((4, lines // 4 + 8, LANES), BF16),
            pltpu.VMEM((KV, lines // 4 + 8, LANES), BF16),
            pltpu.VMEM((4, lines // 4, LANES), BF16),
            pltpu.VMEM((TP, rows, width), F32),
            pltpu.VMEM((KV, 1, LANES), F32),
            pltpu.VMEM((KV // 2, rows, share), BF16),
            pltpu.VMEM((KV, rows, share), BF16),
            pltpu.VMEM((KV // 2, rows, share), BF16),
            pltpu.VMEM((width // LANES, rows, LANES), F32),
            pltpu.VMEM((TP, rows, LANES), F32),
            pltpu.SemaphoreType.REGULAR((2,)),
            dma((8,)),
            dma((2,)),
            dma((9,)),
        ],
        compiler_params=pltpu.CompilerParams(
            collective_id=0, has_side_effects=True, vmem_limit_bytes=64 * 1000 * 1000
        ),
        name="layer",
    )(*args)


def solution(mesh):
    in_specs = (
        P("grp", ("kv", "tp")),
        P("grp", "kv", "tp", None),
        P("grp", "kv", "tp", None),
        P("kv"),
        P("kv", "tp"),
        P("kv", "tp"),
        P("kv", "tp"),
        P("tp"),
        P(),
        P("tp", "kv"),
        P("kv"),
        P("kv", "tp"),
        P("tp", "kv"),
    )
    out_specs = P("grp", ("kv", "tp"))
    fn = functools.partial(body, mesh.shape["kv"], mesh.shape["tp"])
    return jax.shard_map(fn, mesh=mesh, in_specs=in_specs, out_specs=out_specs, check_vma=False)
```

```python
import functools

import jax
import jax.numpy as jnp
from jax import lax
from jax.experimental import pallas as pl
from jax.experimental.pallas import tpu as pltpu
from jax.sharding import PartitionSpec as P

EPS = 1e-06
MESH = pl.DeviceIdType.MESH
F32 = jnp.float32
BF16 = jnp.bfloat16
LANES = 128
LOW = -1e30


def far_first(n):
    def distance(k):
        odd = lax.rem(k, 2)
        return n // 2 + odd * ((k + 1) // 2) - (1 - odd) * (k // 2)

    return distance


def loop(n, step):
    def run(k, carry):
        step(k)
        return carry

    lax.fori_loop(0, n, run, 0)


def three(x):
    high = x.astype(BF16).astype(F32)
    mid = (x - high).astype(BF16).astype(F32)
    return high, mid, x - high - mid


def stacked(rows):
    at = iota((8, LANES), 0)
    out = jnp.zeros((8, LANES), F32)
    for k, row in enumerate(rows):
        out = jnp.where(at == k, row, out)
    return out


class Spread:
    def __init__(self, copy, copy_to, distances, steps, peer, slots):
        self.copy_to, self.distances, self.steps = copy_to, distances, steps
        self.whole = copy(slots, slots, peer)

    def start(self):
        if self.steps is None:
            for d in self.distances:
                self.copy_to(d).start()
        else:
            loop(self.steps, lambda k: self.copy_to(self.distances(k)).start())
        return self

    def arrive(self):
        self.whole.wait_recv()
        self.whole.wait_send()


def iota(shape, dim):
    return lax.broadcasted_iota(jnp.int32, shape, dim)


def dot(a, b):
    return jnp.dot(a, b, preferred_element_type=F32)


def to_lanes(column):
    wide = jnp.broadcast_to(column, (column.shape[0], LANES))
    diagonal = iota(wide.shape, 0) == iota(wide.shape, 1)
    return jnp.sum(jnp.where(diagonal, wide, 0.0), axis=0, keepdims=True)


def to_rows(row, rows):
    wide = jnp.broadcast_to(row, (rows, LANES))
    diagonal = iota(wide.shape, 0) == iota(wide.shape, 1)
    return jnp.sum(jnp.where(diagonal, wide, 0.0), axis=1, keepdims=True)


def kernel(
    KV,
    TP,
    res_h,
    keys_h,
    values_h,
    ng_h,
    wq_h,
    wk_h,
    wv_h,
    lam_h,
    hg_h,
    wo_h,
    mg_h,
    wu_h,
    wd_h,
    out_ref,
    res,
    keys,
    values,
    ng,
    wp,
    lam,
    hg,
    wo,
    mg,
    wu,
    wd,
    abuf,
    qsend,
    qbuf,
    lined_s,
    wsend,
    wbuf,
    nbuf,
    dbuf,
    sqbuf,
    us,
    ur,
    hbuf,
    fs,
    fr,
    ring_sem,
    load_sem,
    send_sem,
    recv_sem,
):
    z = lax.axis_index("kv")
    t = lax.axis_index("tp")
    rows = res_h.shape[0]
    piece = res_h.shape[1]
    per_tile = LANES // piece
    width = wo.shape[1]
    D = KV * width
    qcols = wq_h.shape[1]
    heads = qcols // LANES
    half = LANES // 2
    maps = heads * 2
    lines = rows * maps

    def load(src, dst, k):
        copy = pltpu.make_async_copy(src, dst, load_sem.at[k])
        copy.start()
        return copy

    ld_res = load(res_h, res, 0)
    barrier = pltpu.get_barrier_semaphore()
    def greet(k):
        peer = lax.rem(t + k + 1, TP)
        pl.semaphore_signal(barrier, inc=1, device_id={"tp": peer}, device_id_type=MESH)

    loop(TP - 1, greet)

    def both_ways(sem, d):
        for u in (d, KV - d):
            peer = lax.rem(z + u, KV)
            pl.semaphore_signal(sem, inc=1, device_id={"kv": peer}, device_id_type=MESH)

    both_ways(barrier, 1)
    both_ways(barrier, 2)
    ld_ng = load(ng_h, ng, 1)
    ld_wq = load(wq_h, wp.at[:, 0:qcols], 2)
    ld_wk = load(wk_h, wp.at[:, qcols : qcols + LANES], 3)
    ld_wv = load(wv_h, wp.at[:, qcols + LANES : qcols + 2 * LANES], 4)

    def spread(src_of, dst, buf, ssem, rsem, axis, distances=None):
        me, n = (z, KV) if axis == "kv" else (t, TP)
        steps = n - 1 if distances is None else None
        count = n - 1 if distances is None else len(distances)

        def copy(src, dst, peer):
            return pltpu.make_async_remote_copy(
                src_ref=src,
                dst_ref=dst,
                send_sem=ssem,
                recv_sem=rsem,
                device_id={axis: peer},
                device_id_type=MESH,
            )

        def copy_to(d):
            peer = lax.rem(me + d, n)
            return copy(src_of(peer), dst, peer)

        order = far_first(n) if distances is None else distances
        slots = buf.at[pl.ds(0, count)]
        return Spread(copy, copy_to, order, steps, lax.rem(me + 1, n), slots)

    ld_res.wait()
    own_piece = res[...].astype(F32)
    tiled = jnp.concatenate([own_piece] * per_tile, axis=1)
    at = iota(tiled.shape, 1) // piece == lax.rem(t, per_tile)
    abuf[t] = jnp.where(at, tiled, 0.0).astype(BF16)
    pl.semaphore_wait(barrier, TP - 1 + 4)
    a_copies = spread(lambda peer: abuf.at[t], abuf.at[t], abuf, send_sem.at[0], recv_sem.at[0], "tp").start()
    both_ways(ring_sem.at[0], 2)
    pl.semaphore_wait(ring_sem.at[0], 2)
    both_ways(ring_sem.at[1], 4)
    a_copies.arrive()
    block = jnp.concatenate(
        [
            sum(abuf[k * per_tile + j].astype(F32) for j in range(per_tile))
            for k in range(TP // per_tile)
        ],
        axis=1,
    )
    ld_ng.wait()
    gain = jnp.concatenate([ng[k : k + 1, :] for k in range(width // LANES)], axis=1).astype(F32)
    scaled = (block * gain).astype(BF16)
    ld_wq.wait()
    ld_wk.wait()
    ld_wv.wait()
    proj = dot(scaled, wp[...])
    square = to_lanes(jnp.sum(block * block, axis=1, keepdims=True))
    extra = stacked((square, square, *three(square)))
    at = iota((8, LANES), 0)
    for j in range(KV):
        for g in range(heads):
            qsend[j, g * rows : (g + 1) * rows, :] = proj[:, g * LANES : (g + 1) * LANES].astype(BF16)
        key_row = proj[j : j + 1, qcols : qcols + LANES]
        value_row = proj[j : j + 1, qcols + LANES :]
        last = jnp.where(at == 0, key_row, jnp.where(at == 1, value_row, extra))
        qsend[j, heads * rows :, :] = last.astype(BF16)
    qbuf[z] = qsend[z]
    pl.semaphore_wait(ring_sem.at[1], 2)
    q_copies = spread(lambda peer: qsend.at[peer], qbuf.at[z], qbuf, send_sem.at[0], recv_sem.at[1], "kv").start()
    ld_keys = load(keys_h, keys, 0)
    ld_values = load(values_h, values, 1)
    ld_lam = load(lam_h, lam, 2)
    ld_hg = load(hg_h, hg, 3)
    ld_wo = load(wo_h, wo, 4)
    ld_mg = load(mg_h, mg, 5)
    ld_wu = load(wu_h, wu, 6)
    ld_wd = load(wd_h, wd, 7)
    q_copies.arrive()
    q_sum = qbuf[0].astype(F32)
    for j in range(1, KV):
        q_sum = q_sum + qbuf[j].astype(F32)
    r_sum = q_sum[heads * rows :]
    inv_lanes = lax.rsqrt((r_sum[2:3] + r_sum[3:4] + r_sum[4:5]) / D + EPS)
    inv_own = jnp.sum(
        jnp.where(iota(inv_lanes.shape, 1) == z, inv_lanes, 0.0), axis=1, keepdims=True
    )
    new_key = (inv_own * r_sum[0:1]).astype(BF16).astype(F32)
    new_value = (inv_own * r_sum[1:2]).astype(BF16).astype(F32)
    inv_rows = to_rows(inv_lanes, rows)

    lane = iota((rows, LANES), 1)
    for g in range(heads):
        head = (inv_rows * q_sum[g * rows : (g + 1) * rows]).astype(BF16)
        head = head.astype(F32) * (1.0 / half**0.5)
        for c in range(2):
            lined_s[pl.ds(2 * g + c, rows, stride=maps), :] = jnp.where(lane // half == c, head, 0.0)
    lined = lined_s[...]

    ld_keys.wait()
    ld_values.wait()
    tops, totals, sums = [], [], []
    seqs = 8 // maps
    group = iota((8, LANES), 0) // maps
    for p in range(lines // 8):
        qp = lined[8 * p : 8 * p + 8, :]
        wide = jnp.concatenate([jnp.where(group == k, qp, 0.0) for k in range(seqs)], axis=1)
        wide_keys = jnp.concatenate([keys[seqs * p + k] for k in range(seqs)], axis=1)
        scores = lax.dot_general(
            wide.astype(BF16), wide_keys, (((1,), (1,)), ((), ())), preferred_element_type=F32
        )
        top = jnp.max(scores, axis=1, keepdims=True)
        expo = jnp.exp(scores - top)
        wide_values = jnp.concatenate([values[seqs * p + k] for k in range(seqs)], axis=1)
        part = dot(expo.astype(BF16), wide_values)
        weighted = part[:, 0:LANES]
        for k in range(1, seqs):
            weighted = jnp.where(group == k, part[:, k * LANES : (k + 1) * LANES], weighted)
        tops.append(top)
        totals.append(jnp.sum(expo, axis=1, keepdims=True))
        sums.append(weighted)
    top = jnp.concatenate(tops, axis=0)
    total = jnp.concatenate(totals, axis=0)
    weighted = jnp.concatenate(sums, axis=0)
    own = jnp.sum(lined * new_key, axis=1, keepdims=True)
    own = jnp.where(iota(own.shape, 0) // maps == z, own, LOW)
    new_top = jnp.maximum(top, own)
    old_part = jnp.exp(top - new_top)
    own_part = jnp.exp(own - new_top)
    total = total * old_part + own_part
    weighted = weighted * old_part + own_part * new_value
    quarter = lines // 4
    mine = lax.rem(z, 4)
    for c in range(4):
        at = slice(c * quarter, (c + 1) * quarter)
        wsend[c, 0:quarter, :] = weighted[at].astype(BF16)
        both = stacked((*three(to_lanes(new_top[at])), *three(to_lanes(total[at]))))
        wsend[c, quarter:, :] = both.astype(BF16)
    wbuf[z] = wsend[mine]
    w_copies = spread(lambda peer: wsend.at[lax.rem(peer, 4)], wbuf.at[z], wbuf, send_sem.at[0], recv_sem.at[2], "kv").start()
    w_copies.arrive()
    tails = [wbuf[j, quarter:, :].astype(F32) for j in range(KV)]
    ml = jnp.concatenate([x[0:1] + x[1:2] + x[2:3] for x in tails], axis=0)
    totals = jnp.concatenate([x[3:4] + x[4:5] + x[5:6] for x in tails], axis=0)
    shares = jnp.exp(ml - jnp.max(ml, axis=0, keepdims=True))
    grand = jnp.sum(shares * totals, axis=0, keepdims=True)
    in_use = iota(ml.shape, 1) < quarter
    shares = jnp.where(in_use, shares / jnp.where(in_use[0:1], grand, 1.0), 0.0)
    columns = jnp.transpose(shares)
    attended = columns[0:quarter, 0:1] * wbuf[0, 0:quarter, :].astype(F32)
    for j in range(1, KV):
        attended = attended + columns[0:quarter, j : j + 1] * wbuf[j, 0:quarter, :].astype(F32)
    ld_lam.wait()
    ld_hg.wait()
    lambdas = lam[0:1, 0:1]
    for g in range(1, heads):
        lambdas = jnp.where(
            lax.rem(iota((quarter, 1), 0), maps) // 2 == g, lam[0:1, g : g + 1], lambdas
        )
    diff = attended - lambdas * pltpu.roll(attended, quarter - 1, 0)
    normed = (
        diff
        * lax.rsqrt(jnp.mean(diff * diff, axis=1, keepdims=True) + EPS)
        * hg[...].astype(F32)
    ).astype(BF16)
    nbuf[mine] = normed
    spread(lambda peer: nbuf.at[mine], nbuf.at[mine], nbuf, send_sem.at[0], recv_sem.at[3], "kv", (2, 1, KV - 1)).start().arrive()
    for c in range(4):
        lined_s[c * quarter : (c + 1) * quarter, :] = nbuf[c].astype(F32)
    outs = [lined_s[pl.ds(2 * g, rows, stride=maps), :] for g in range(heads)]
    heads_out = jnp.concatenate(outs, axis=1).astype(BF16)
    ld_wo.wait()
    dbuf[t] = dot(heads_out, wo[...]).astype(BF16)
    spread(lambda peer: dbuf.at[t], dbuf.at[t], dbuf, send_sem.at[0], recv_sem.at[4], "tp").start().arrive()
    projected = dbuf[0].astype(F32)
    for j in range(1, TP):
        projected = projected + dbuf[j].astype(F32)
    mixed = (block + projected).astype(BF16).astype(F32)
    sqbuf[z] = to_lanes(jnp.sum(mixed * mixed, axis=1, keepdims=True))
    ld_mg.wait()
    gain2 = jnp.concatenate([mg[k : k + 1, :] for k in range(width // LANES)], axis=1).astype(F32)
    scaled2 = (mixed * gain2).astype(BF16)
    ld_wu.wait()
    up = dot(scaled2, wu[...])
    owners = KV // 2
    owned = lax.rem(z, owners)
    share_width = up.shape[1] // owners
    for j in range(owners):
        us[j] = up[:, j * share_width : (j + 1) * share_width].astype(BF16)
    ur[z] = us[owned]
    u_copies = spread(lambda peer: us.at[lax.rem(peer, owners)], ur.at[z], ur, send_sem.at[0], recv_sem.at[5], "kv").start()
    u_copies.arrive()
    up_sum = ur[0].astype(F32)
    for j in range(1, KV):
        up_sum = up_sum + ur[j].astype(F32)
    act = jnp.maximum(up_sum, 0.0)
    hbuf[owned] = (act * act).astype(BF16)
    near = [owners // 2]
    for d in range(owners // 2 - 1, 0, -1):
        near += [d, KV - d]
    h_copies = spread(lambda peer: hbuf.at[owned], hbuf.at[owned], hbuf, send_sem.at[0], recv_sem.at[7], "kv", near).start()
    s_copies = spread(lambda peer: sqbuf.at[z], sqbuf.at[z], sqbuf, send_sem.at[1], recv_sem.at[6], "kv").start()
    h_copies.arrive()
    hidden = jnp.concatenate([hbuf[j] for j in range(owners)], axis=1)
    ld_wd.wait()
    down = dot(hidden, wd[...])
    for k in range(width // LANES):
        fs[k] = down[:, k * LANES : (k + 1) * LANES]
    fr[t] = fs[t // per_tile]
    f_copies = spread(lambda peer: fs.at[peer // per_tile], fr.at[t], fr, send_sem.at[0], recv_sem.at[8], "tp").start()
    s_copies.arrive()
    square2 = sqbuf[0]
    for j in range(1, KV):
        square2 = square2 + sqbuf[j]
    inv2 = to_rows(1.0 / (square2 / D + EPS), rows)
    f_copies.arrive()
    y = fr[0]
    for j in range(1, TP):
        y = y + fr[j]
    y = inv2 * y
    for k in range(width // LANES):
        y = y + jnp.where(t // per_tile == k, mixed[:, k * LANES : (k + 1) * LANES], 0.0)
    result = y[:, 0:piece]
    for k in range(1, per_tile):
        result = jnp.where(lax.rem(t, per_tile) == k, y[:, k * piece : (k + 1) * piece], result)
    out_ref[...] = result.astype(out_ref.dtype)


def body(
    KV,
    TP,
    residual,
    cache_keys,
    cache_values,
    norm_gain,
    query_weight,
    key_weight,
    value_weight,
    head_lambda,
    head_gain,
    out_weight,
    mixer_gain,
    up_weight,
    down_weight,
):
    rows, piece = residual.shape
    positions, depth = cache_keys.shape[1], cache_keys.shape[3]
    width = out_weight.shape[1]
    qcols = query_weight.shape[1]
    lines = rows * qcols * 2 // LANES
    share = up_weight.shape[1] * 2 // KV
    any_spec = pl.BlockSpec(memory_space=pl.ANY)
    dma = pltpu.SemaphoreType.DMA
    keys = cache_keys.reshape(rows, positions, depth)
    values = cache_values.reshape(rows, positions, depth)
    args = (
        residual,
        keys,
        values,
        norm_gain.reshape(width // LANES, LANES),
        query_weight,
        key_weight,
        value_weight,
        head_lambda.reshape(1, -1),
        head_gain.reshape(1, -1),
        out_weight,
        mixer_gain.reshape(width // LANES, LANES),
        up_weight,
        down_weight,
    )
    return pl.pallas_call(
        functools.partial(kernel, KV, TP),
        out_shape=jax.ShapeDtypeStruct((rows, piece), residual.dtype),
        in_specs=[any_spec] * len(args),
        out_specs=pl.BlockSpec(memory_space=pltpu.VMEM),
        scratch_shapes=[
            pltpu.VMEM((rows, piece), BF16),
            pltpu.VMEM(keys.shape, BF16),
            pltpu.VMEM(values.shape, BF16),
            pltpu.VMEM((width // LANES, LANES), BF16),
            pltpu.VMEM((width, qcols + 2 * LANES), BF16),
            pltpu.VMEM((1, head_lambda.shape[0]), F32),
            pltpu.VMEM((1, head_gain.shape[0]), BF16),
            pltpu.VMEM(out_weight.shape, BF16),
            pltpu.VMEM((width // LANES, LANES), BF16),
            pltpu.VMEM(up_weight.shape, BF16),
            pltpu.VMEM(down_weight.shape, BF16),
            pltpu.VMEM((TP, rows, LANES), BF16),
            pltpu.VMEM((KV, rows * qcols // LANES + 8, LANES), BF16),
            pltpu.VMEM((KV, rows * qcols // LANES + 8, LANES), BF16),
            pltpu.VMEM((lines, LANES), F32),
            pltpu.VMEM((4, lines // 4 + 8, LANES), BF16),
            pltpu.VMEM((KV, lines // 4 + 8, LANES), BF16),
            pltpu.VMEM((4, lines // 4, LANES), BF16),
            pltpu.VMEM((TP, rows, width), BF16),
            pltpu.VMEM((KV, 1, LANES), F32),
            pltpu.VMEM((KV // 2, rows, share), BF16),
            pltpu.VMEM((KV, rows, share), BF16),
            pltpu.VMEM((KV // 2, rows, share), BF16),
            pltpu.VMEM((width // LANES, rows, LANES), F32),
            pltpu.VMEM((TP, rows, LANES), F32),
            pltpu.SemaphoreType.REGULAR((2,)),
            dma((8,)),
            dma((2,)),
            dma((9,)),
        ],
        compiler_params=pltpu.CompilerParams(
            collective_id=0, has_side_effects=True, vmem_limit_bytes=64 * 1000 * 1000
        ),
        name="layer",
    )(*args)


def solution(mesh):
    in_specs = (
        P("grp", ("kv", "tp")),
        P("grp", "kv", "tp", None),
        P("grp", "kv", "tp", None),
        P("kv"),
        P("kv", "tp"),
        P("kv", "tp"),
        P("kv", "tp"),
        P("tp"),
        P(),
        P("tp", "kv"),
        P("kv"),
        P("kv", "tp"),
        P("tp", "kv"),
    )
    out_specs = P("grp", ("kv", "tp"))
    fn = functools.partial(body, mesh.shape["kv"], mesh.shape["tp"])
    return jax.shard_map(fn, mesh=mesh, in_specs=in_specs, out_specs=out_specs, check_vma=False)
```

```python
import functools

import jax
import jax.numpy as jnp
from jax import lax
from jax.experimental import pallas as pl
from jax.experimental.pallas import tpu as pltpu
from jax.sharding import PartitionSpec as P

EPS = 1e-06
MESH = pl.DeviceIdType.MESH
F32 = jnp.float32
BF16 = jnp.bfloat16
LANES = 128
LOW = -1e30


def far_first(n):
    def distance(k):
        odd = lax.rem(k, 2)
        return n // 2 + odd * ((k + 1) // 2) - (1 - odd) * (k // 2)

    return distance


def loop(n, step):
    def run(k, carry):
        step(k)
        return carry

    lax.fori_loop(0, n, run, 0)


def three(x):
    high = x.astype(BF16).astype(F32)
    mid = (x - high).astype(BF16).astype(F32)
    return high, mid, x - high - mid


def stacked(rows):
    at = iota((8, LANES), 0)
    out = jnp.zeros((8, LANES), F32)
    for k, row in enumerate(rows):
        out = jnp.where(at == k, row, out)
    return out


class Spread:
    def __init__(self, copy, copy_to, distances, steps, peer, slots):
        self.copy_to, self.distances, self.steps = copy_to, distances, steps
        self.whole = lambda: copy(slots, slots, peer)

    def start(self, first=0, last=None):
        if self.steps is None:
            for d in self.distances:
                self.copy_to(d).start()
        else:
            steps = (self.steps if last is None else last) - first
            loop(steps, lambda k: self.copy_to(self.distances(k + first)).start())
        return self

    def arrive(self):
        whole = self.whole()
        whole.wait_recv()
        whole.wait_send()


def iota(shape, dim):
    return lax.broadcasted_iota(jnp.int32, shape, dim)


def dot(a, b):
    return jnp.dot(a, b, preferred_element_type=F32)


def to_lanes(column):
    wide = jnp.broadcast_to(column, (column.shape[0], LANES))
    diagonal = iota(wide.shape, 0) == iota(wide.shape, 1)
    return jnp.sum(jnp.where(diagonal, wide, 0.0), axis=0, keepdims=True)


def to_rows(row, rows):
    wide = jnp.broadcast_to(row, (rows, LANES))
    diagonal = iota(wide.shape, 0) == iota(wide.shape, 1)
    return jnp.sum(jnp.where(diagonal, wide, 0.0), axis=1, keepdims=True)


def kernel(
    KV,
    TP,
    res_h,
    keys_h,
    values_h,
    ng_h,
    wq_h,
    wk_h,
    wv_h,
    lam_h,
    hg_h,
    wo_h,
    mg_h,
    wu_h,
    wd_h,
    out_ref,
    res,
    keys,
    values,
    ng,
    wp,
    lam,
    hg,
    wo,
    mg,
    wu,
    wd,
    abuf,
    qsend,
    qbuf,
    lined_s,
    wsend,
    wbuf,
    nbuf,
    dbuf,
    sqbuf,
    us,
    ur,
    hbuf,
    fs,
    fr,
    ring_sem,
    load_sem,
    send_sem,
    recv_sem,
):
    z = lax.axis_index("kv")
    t = lax.axis_index("tp")
    rows = res_h.shape[0]
    piece = res_h.shape[1]
    per_tile = LANES // piece
    width = wo.shape[1]
    D = KV * width
    qcols = wq_h.shape[1]
    heads = qcols // LANES
    half = LANES // 2
    maps = heads * 2
    lines = rows * maps

    def load(src, dst, k):
        copy = pltpu.make_async_copy(src, dst, load_sem.at[k])
        copy.start()
        return copy

    ld_res = load(res_h, res, 0)
    barrier = pltpu.get_barrier_semaphore()
    def greet(k):
        peer = lax.rem(t + k + 1, TP)
        pl.semaphore_signal(barrier, inc=1, device_id={"tp": peer}, device_id_type=MESH)

    loop(TP - 1, greet)

    def both_ways(sem, d):
        for u in (d, KV - d):
            peer = lax.rem(z + u, KV)
            pl.semaphore_signal(sem, inc=1, device_id={"kv": peer}, device_id_type=MESH)

    both_ways(barrier, 1)
    both_ways(barrier, 2)
    ld_ng = load(ng_h, ng, 1)
    ld_wq = load(wq_h, wp.at[:, 0:qcols], 2)
    ld_wk = load(wk_h, wp.at[:, qcols : qcols + LANES], 3)
    ld_wv = load(wv_h, wp.at[:, qcols + LANES : qcols + 2 * LANES], 4)

    def spread(src_of, dst, buf, ssem, rsem, axis, distances=None):
        me, n = (z, KV) if axis == "kv" else (t, TP)
        steps = n - 1 if distances is None else None
        count = n - 1 if distances is None else len(distances)

        def copy(src, dst, peer):
            return pltpu.make_async_remote_copy(
                src_ref=src,
                dst_ref=dst,
                send_sem=ssem,
                recv_sem=rsem,
                device_id={axis: peer},
                device_id_type=MESH,
            )

        def copy_to(d):
            peer = lax.rem(me + d, n)
            return copy(src_of(peer), dst, peer)

        order = far_first(n) if distances is None else distances
        slots = buf.at[pl.ds(0, count)]
        return Spread(copy, copy_to, order, steps, lax.rem(me + 1, n), slots)

    ld_res.wait()
    own_piece = res[...].astype(F32)
    tiled = jnp.concatenate([own_piece] * per_tile, axis=1)
    at = iota(tiled.shape, 1) // piece == lax.rem(t, per_tile)
    abuf[t] = jnp.where(at, tiled, 0.0).astype(BF16)
    pl.semaphore_wait(barrier, TP - 1 + 4)
    a_copies = spread(lambda peer: abuf.at[t], abuf.at[t], abuf, send_sem.at[0], recv_sem.at[0], "tp").start()
    both_ways(ring_sem.at[0], 2)
    pl.semaphore_wait(ring_sem.at[0], 2)
    both_ways(ring_sem.at[1], 4)
    a_copies.arrive()
    block = jnp.concatenate(
        [
            sum(abuf[k * per_tile + j].astype(F32) for j in range(per_tile))
            for k in range(TP // per_tile)
        ],
        axis=1,
    )
    ld_ng.wait()
    gain = jnp.concatenate([ng[k : k + 1, :] for k in range(width // LANES)], axis=1).astype(F32)
    scaled = (block * gain).astype(BF16)
    ld_wq.wait()
    ld_wk.wait()
    ld_wv.wait()
    proj = dot(scaled, wp[...])
    square = to_lanes(jnp.sum(block * block, axis=1, keepdims=True))
    extra = stacked((square, square, *three(square)))
    at = iota((8, LANES), 0)
    for j in range(KV):
        for g in range(heads):
            qsend[j, g * rows : (g + 1) * rows, :] = proj[:, g * LANES : (g + 1) * LANES].astype(BF16)
        key_row = proj[j : j + 1, qcols : qcols + LANES]
        value_row = proj[j : j + 1, qcols + LANES :]
        last = jnp.where(at == 0, key_row, jnp.where(at == 1, value_row, extra))
        qsend[j, heads * rows :, :] = last.astype(BF16)
    qbuf[z] = qsend[z]
    q_copies = spread(lambda peer: qsend.at[peer], qbuf.at[z], qbuf, send_sem.at[0], recv_sem.at[1], "kv")
    far = KV // 2 - 1
    q_copies.start(far)
    pl.semaphore_wait(ring_sem.at[1], 2)
    q_copies.start(0, far)
    ld_keys = load(keys_h, keys, 0)
    ld_values = load(values_h, values, 1)
    ld_lam = load(lam_h, lam, 2)
    ld_hg = load(hg_h, hg, 3)
    ld_wo = load(wo_h, wo, 4)
    ld_mg = load(mg_h, mg, 5)
    ld_wu = load(wu_h, wu, 6)
    ld_wd = load(wd_h, wd, 7)
    q_copies.arrive()
    q_sum = qbuf[0].astype(F32)
    for j in range(1, KV):
        q_sum = q_sum + qbuf[j].astype(F32)
    r_sum = q_sum[heads * rows :]
    inv_lanes = lax.rsqrt((r_sum[2:3] + r_sum[3:4] + r_sum[4:5]) / D + EPS)
    inv_own = jnp.sum(
        jnp.where(iota(inv_lanes.shape, 1) == z, inv_lanes, 0.0), axis=1, keepdims=True
    )
    new_key = (inv_own * r_sum[0:1]).astype(BF16).astype(F32)
    new_value = (inv_own * r_sum[1:2]).astype(BF16).astype(F32)
    inv_rows = to_rows(inv_lanes, rows)

    lane = iota((rows, LANES), 1)
    for g in range(heads):
        head = (inv_rows * q_sum[g * rows : (g + 1) * rows]).astype(BF16)
        head = head.astype(F32) * (1.0 / half**0.5)
        for c in range(2):
            lined_s[pl.ds(2 * g + c, rows, stride=maps), :] = jnp.where(lane // half == c, head, 0.0)

    ld_keys.wait()
    ld_values.wait()
    seqs = 8 // maps
    group = iota((8, LANES), 0) // maps
    quarter = lines // 4
    mine = lax.rem(z, 4)
    for r in (0, 3, 1, 2):
        part_of = lax.rem(mine + r, 4)
        tops, totals, sums = [], [], []
        for u in range(quarter // 8):
            p = part_of * (quarter // 8) + u
            qp = lined_s[pl.ds(pl.multiple_of(8 * p, 8), 8), :]
            wide = jnp.concatenate([jnp.where(group == k, qp, 0.0) for k in range(seqs)], axis=1)
            wide_keys = jnp.concatenate([keys[seqs * p + k] for k in range(seqs)], axis=1)
            scores = lax.dot_general(
                wide.astype(BF16), wide_keys, (((1,), (1,)), ((), ())), preferred_element_type=F32
            )
            top = jnp.max(scores, axis=1, keepdims=True)
            expo = jnp.exp(scores - top)
            wide_values = jnp.concatenate([values[seqs * p + k] for k in range(seqs)], axis=1)
            part = dot(expo.astype(BF16), wide_values)
            weighted = part[:, 0:LANES]
            for k in range(1, seqs):
                weighted = jnp.where(group == k, part[:, k * LANES : (k + 1) * LANES], weighted)
            tops.append(top)
            totals.append(jnp.sum(expo, axis=1, keepdims=True))
            sums.append(weighted)
        top = jnp.concatenate(tops, axis=0)
        total = jnp.concatenate(totals, axis=0)
        weighted = jnp.concatenate(sums, axis=0)
        queries = lined_s[pl.ds(pl.multiple_of(quarter * part_of, quarter), quarter), :]
        own = jnp.sum(queries * new_key, axis=1, keepdims=True)
        sequence = part_of * (quarter // maps) + iota(own.shape, 0) // maps
        own = jnp.where(sequence == z, own, LOW)
        new_top = jnp.maximum(top, own)
        old_part = jnp.exp(top - new_top)
        own_part = jnp.exp(own - new_top)
        total = total * old_part + own_part
        weighted = weighted * old_part + own_part * new_value
        wsend[r, 0:quarter, :] = weighted.astype(BF16)
        both = stacked((*three(to_lanes(new_top)), *three(to_lanes(total))))
        wsend[r, quarter:, :] = both.astype(BF16)
        reach = sorted(range(r if r else 4, KV, 4), key=lambda d: -min(d, KV - d))
        spread(
            lambda peer: wsend.at[r], wbuf.at[z], wbuf, send_sem.at[0], recv_sem.at[2], "kv", reach
        ).start()
    wbuf[z] = wsend[0]
    w_copies = spread(lambda peer: wsend.at[0], wbuf.at[z], wbuf, send_sem.at[0], recv_sem.at[2], "kv")
    w_copies.arrive()
    tails = [wbuf[j, quarter:, :].astype(F32) for j in range(KV)]
    ml = jnp.concatenate([x[0:1] + x[1:2] + x[2:3] for x in tails], axis=0)
    totals = jnp.concatenate([x[3:4] + x[4:5] + x[5:6] for x in tails], axis=0)
    shares = jnp.exp(ml - jnp.max(ml, axis=0, keepdims=True))
    grand = jnp.sum(shares * totals, axis=0, keepdims=True)
    in_use = iota(ml.shape, 1) < quarter
    shares = jnp.where(in_use, shares / jnp.where(in_use[0:1], grand, 1.0), 0.0)
    columns = jnp.transpose(shares)
    attended = columns[0:quarter, 0:1] * wbuf[0, 0:quarter, :].astype(F32)
    for j in range(1, KV):
        attended = attended + columns[0:quarter, j : j + 1] * wbuf[j, 0:quarter, :].astype(F32)
    ld_lam.wait()
    ld_hg.wait()
    lambdas = lam[0:1, 0:1]
    for g in range(1, heads):
        lambdas = jnp.where(
            lax.rem(iota((quarter, 1), 0), maps) // 2 == g, lam[0:1, g : g + 1], lambdas
        )
    diff = attended - lambdas * pltpu.roll(attended, quarter - 1, 0)
    normed = (
        diff
        * lax.rsqrt(jnp.mean(diff * diff, axis=1, keepdims=True) + EPS)
        * hg[...].astype(F32)
    ).astype(BF16)
    nbuf[mine] = normed
    spread(lambda peer: nbuf.at[mine], nbuf.at[mine], nbuf, send_sem.at[0], recv_sem.at[3], "kv", (2, 1, KV - 1)).start().arrive()
    for c in range(4):
        lined_s[c * quarter : (c + 1) * quarter, :] = nbuf[c].astype(F32)
    outs = [lined_s[pl.ds(2 * g, rows, stride=maps), :] for g in range(heads)]
    heads_out = jnp.concatenate(outs, axis=1).astype(BF16)
    ld_wo.wait()
    dbuf[t] = dot(heads_out, wo[...]).astype(BF16)
    spread(lambda peer: dbuf.at[t], dbuf.at[t], dbuf, send_sem.at[0], recv_sem.at[4], "tp").start().arrive()
    projected = dbuf[0].astype(F32)
    for j in range(1, TP):
        projected = projected + dbuf[j].astype(F32)
    mixed = (block + projected).astype(BF16).astype(F32)
    sqbuf[z] = to_lanes(jnp.sum(mixed * mixed, axis=1, keepdims=True))
    ld_mg.wait()
    gain2 = jnp.concatenate([mg[k : k + 1, :] for k in range(width // LANES)], axis=1).astype(F32)
    scaled2 = (mixed * gain2).astype(BF16)
    ld_wu.wait()
    up = dot(scaled2, wu[...])
    owners = KV // 2
    owned = lax.rem(z, owners)
    share_width = up.shape[1] // owners
    for j in range(owners):
        us[j] = up[:, j * share_width : (j + 1) * share_width].astype(BF16)
    ur[z] = us[owned]
    u_copies = spread(lambda peer: us.at[lax.rem(peer, owners)], ur.at[z], ur, send_sem.at[0], recv_sem.at[5], "kv").start()
    u_copies.arrive()
    up_sum = ur[0].astype(F32)
    for j in range(1, KV):
        up_sum = up_sum + ur[j].astype(F32)
    act = jnp.maximum(up_sum, 0.0)
    hbuf[owned] = (act * act).astype(BF16)
    near = [owners // 2]
    for d in range(owners // 2 - 1, 0, -1):
        near += [d, KV - d]
    h_copies = spread(lambda peer: hbuf.at[owned], hbuf.at[owned], hbuf, send_sem.at[0], recv_sem.at[7], "kv", near).start()
    s_copies = spread(lambda peer: sqbuf.at[z], sqbuf.at[z], sqbuf, send_sem.at[1], recv_sem.at[6], "kv").start()
    h_copies.arrive()
    hidden = jnp.concatenate([hbuf[j] for j in range(owners)], axis=1)
    ld_wd.wait()
    down = dot(hidden, wd[...])
    for k in range(width // LANES):
        fs[k] = down[:, k * LANES : (k + 1) * LANES]
    fr[t] = fs[t // per_tile]
    f_copies = spread(lambda peer: fs.at[peer // per_tile], fr.at[t], fr, send_sem.at[0], recv_sem.at[8], "tp").start()
    s_copies.arrive()
    square2 = sqbuf[0]
    for j in range(1, KV):
        square2 = square2 + sqbuf[j]
    inv2 = to_rows(1.0 / (square2 / D + EPS), rows)
    f_copies.arrive()
    y = fr[0]
    for j in range(1, TP):
        y = y + fr[j]
    y = inv2 * y
    for k in range(width // LANES):
        y = y + jnp.where(t // per_tile == k, mixed[:, k * LANES : (k + 1) * LANES], 0.0)
    result = y[:, 0:piece]
    for k in range(1, per_tile):
        result = jnp.where(lax.rem(t, per_tile) == k, y[:, k * piece : (k + 1) * piece], result)
    out_ref[...] = result.astype(out_ref.dtype)


def body(
    KV,
    TP,
    residual,
    cache_keys,
    cache_values,
    norm_gain,
    query_weight,
    key_weight,
    value_weight,
    head_lambda,
    head_gain,
    out_weight,
    mixer_gain,
    up_weight,
    down_weight,
):
    rows, piece = residual.shape
    positions, depth = cache_keys.shape[1], cache_keys.shape[3]
    width = out_weight.shape[1]
    qcols = query_weight.shape[1]
    lines = rows * qcols * 2 // LANES
    share = up_weight.shape[1] * 2 // KV
    any_spec = pl.BlockSpec(memory_space=pl.ANY)
    dma = pltpu.SemaphoreType.DMA
    keys = cache_keys.reshape(rows, positions, depth)
    values = cache_values.reshape(rows, positions, depth)
    args = (
        residual,
        keys,
        values,
        norm_gain.reshape(width // LANES, LANES),
        query_weight,
        key_weight,
        value_weight,
        head_lambda.reshape(1, -1),
        head_gain.reshape(1, -1),
        out_weight,
        mixer_gain.reshape(width // LANES, LANES),
        up_weight,
        down_weight,
    )
    return pl.pallas_call(
        functools.partial(kernel, KV, TP),
        out_shape=jax.ShapeDtypeStruct((rows, piece), residual.dtype),
        in_specs=[any_spec] * len(args),
        out_specs=pl.BlockSpec(memory_space=pltpu.VMEM),
        scratch_shapes=[
            pltpu.VMEM((rows, piece), BF16),
            pltpu.VMEM(keys.shape, BF16),
            pltpu.VMEM(values.shape, BF16),
            pltpu.VMEM((width // LANES, LANES), BF16),
            pltpu.VMEM((width, qcols + 2 * LANES), BF16),
            pltpu.VMEM((1, head_lambda.shape[0]), F32),
            pltpu.VMEM((1, head_gain.shape[0]), BF16),
            pltpu.VMEM(out_weight.shape, BF16),
            pltpu.VMEM((width // LANES, LANES), BF16),
            pltpu.VMEM(up_weight.shape, BF16),
            pltpu.VMEM(down_weight.shape, BF16),
            pltpu.VMEM((TP, rows, LANES), BF16),
            pltpu.VMEM((KV, rows * qcols // LANES + 8, LANES), BF16),
            pltpu.VMEM((KV, rows * qcols // LANES + 8, LANES), BF16),
            pltpu.VMEM((lines, LANES), F32),
            pltpu.VMEM((4, lines // 4 + 8, LANES), BF16),
            pltpu.VMEM((KV, lines // 4 + 8, LANES), BF16),
            pltpu.VMEM((4, lines // 4, LANES), BF16),
            pltpu.VMEM((TP, rows, width), BF16),
            pltpu.VMEM((KV, 1, LANES), F32),
            pltpu.VMEM((KV // 2, rows, share), BF16),
            pltpu.VMEM((KV, rows, share), BF16),
            pltpu.VMEM((KV // 2, rows, share), BF16),
            pltpu.VMEM((width // LANES, rows, LANES), F32),
            pltpu.VMEM((TP, rows, LANES), F32),
            pltpu.SemaphoreType.REGULAR((2,)),
            dma((8,)),
            dma((2,)),
            dma((9,)),
        ],
        compiler_params=pltpu.CompilerParams(
            collective_id=0, has_side_effects=True, vmem_limit_bytes=64 * 1000 * 1000
        ),
        name="layer",
    )(*args)


def solution(mesh):
    in_specs = (
        P("grp", ("kv", "tp")),
        P("grp", "kv", "tp", None),
        P("grp", "kv", "tp", None),
        P("kv"),
        P("kv", "tp"),
        P("kv", "tp"),
        P("kv", "tp"),
        P("tp"),
        P(),
        P("tp", "kv"),
        P("kv"),
        P("kv", "tp"),
        P("tp", "kv"),
    )
    out_specs = P("grp", ("kv", "tp"))
    fn = functools.partial(body, mesh.shape["kv"], mesh.shape["tp"])
    return jax.shard_map(fn, mesh=mesh, in_specs=in_specs, out_specs=out_specs, check_vma=False)
```

```python
import functools

import jax
import jax.numpy as jnp
from jax import lax
from jax.experimental import pallas as pl
from jax.experimental.pallas import tpu as pltpu
from jax.sharding import PartitionSpec as P

EPS = 1e-06
MESH = pl.DeviceIdType.MESH
F32 = jnp.float32
BF16 = jnp.bfloat16
LANES = 128
LOW = -1e30


def far_first(n):
    def distance(k):
        odd = lax.rem(k, 2)
        return n // 2 + odd * ((k + 1) // 2) - (1 - odd) * (k // 2)

    return distance


def loop(n, step):
    def run(k, carry):
        step(k)
        return carry

    lax.fori_loop(0, n, run, 0)


def three(x):
    high = x.astype(BF16).astype(F32)
    mid = (x - high).astype(BF16).astype(F32)
    return high, mid, x - high - mid


def stacked(rows):
    at = iota((8, LANES), 0)
    out = jnp.zeros((8, LANES), F32)
    for k, row in enumerate(rows):
        out = jnp.where(at == k, row, out)
    return out


class Spread:
    def __init__(self, copy, copy_to, distances, steps, peer, slots):
        self.copy_to, self.distances, self.steps = copy_to, distances, steps
        self.whole = lambda: copy(slots, slots, peer)

    def start(self):
        if self.steps is None:
            for d in self.distances:
                self.copy_to(d).start()
        else:
            loop(self.steps, lambda k: self.copy_to(self.distances(k)).start())
        return self

    def arrive(self):
        whole = self.whole()
        whole.wait_recv()
        whole.wait_send()


def iota(shape, dim):
    return lax.broadcasted_iota(jnp.int32, shape, dim)


def dot(a, b):
    return jnp.dot(a, b, preferred_element_type=F32)


def to_lanes(column):
    wide = jnp.broadcast_to(column, (column.shape[0], LANES))
    diagonal = iota(wide.shape, 0) == iota(wide.shape, 1)
    return jnp.sum(jnp.where(diagonal, wide, 0.0), axis=0, keepdims=True)


def to_rows(row, rows):
    wide = jnp.broadcast_to(row, (rows, LANES))
    diagonal = iota(wide.shape, 0) == iota(wide.shape, 1)
    return jnp.sum(jnp.where(diagonal, wide, 0.0), axis=1, keepdims=True)


def kernel(
    KV,
    TP,
    res_h,
    keys_h,
    values_h,
    ng_h,
    wq_h,
    wk_h,
    wv_h,
    lam_h,
    hg_h,
    wo_h,
    mg_h,
    wu_h,
    wd_h,
    out_ref,
    res,
    keys,
    values,
    ng,
    wp,
    lam,
    hg,
    wo,
    mg,
    wu,
    wd,
    abuf,
    psend,
    precv,
    qsend,
    qbuf,
    lined_s,
    wsend,
    wbuf,
    nbuf,
    dbuf,
    sqbuf,
    us,
    ur,
    hbuf,
    fs,
    fr,
    ring_sem,
    load_sem,
    send_sem,
    recv_sem,
):
    z = lax.axis_index("kv")
    t = lax.axis_index("tp")
    rows = res_h.shape[0]
    piece = res_h.shape[1]
    per_tile = LANES // piece
    width = wo.shape[1]
    D = KV * width
    qcols = wq_h.shape[1]
    heads = qcols // LANES
    half = LANES // 2
    maps = heads * 2
    lines = rows * maps

    def load(src, dst, k):
        copy = pltpu.make_async_copy(src, dst, load_sem.at[k])
        copy.start()
        return copy

    ld_res = load(res_h, res, 0)
    barrier = pltpu.get_barrier_semaphore()
    def greet(k):
        peer = lax.rem(t + k + 1, TP)
        pl.semaphore_signal(barrier, inc=1, device_id={"tp": peer}, device_id_type=MESH)

    loop(TP - 1, greet)

    def both_ways(sem, d):
        for u in (d, KV - d):
            peer = lax.rem(z + u, KV)
            pl.semaphore_signal(sem, inc=1, device_id={"kv": peer}, device_id_type=MESH)

    both_ways(barrier, 1)
    both_ways(barrier, 2)
    ld_ng = load(ng_h, ng, 1)
    ld_wq = load(wq_h, wp.at[:, 0:qcols], 2)
    ld_wk = load(wk_h, wp.at[:, qcols : qcols + LANES], 3)
    ld_wv = load(wv_h, wp.at[:, qcols + LANES : qcols + 2 * LANES], 4)

    def spread(src_of, dst, buf, ssem, rsem, axis, distances=None):
        me, n = (z, KV) if axis == "kv" else (t, TP)
        steps = n - 1 if distances is None else None
        count = n - 1 if distances is None else len(distances)

        def copy(src, dst, peer):
            return pltpu.make_async_remote_copy(
                src_ref=src,
                dst_ref=dst,
                send_sem=ssem,
                recv_sem=rsem,
                device_id={axis: peer},
                device_id_type=MESH,
            )

        def copy_to(d):
            peer = lax.rem(me + d, n)
            return copy(src_of(peer), dst, peer)

        order = far_first(n) if distances is None else distances
        slots = buf.at[pl.ds(0, count)]
        return Spread(copy, copy_to, order, steps, lax.rem(me + 1, n), slots)

    ld_res.wait()
    own_piece = res[...].astype(F32)
    tiled = jnp.concatenate([own_piece] * per_tile, axis=1)
    at = iota(tiled.shape, 1) // piece == lax.rem(t, per_tile)
    abuf[t] = jnp.where(at, tiled, 0.0).astype(BF16)
    pl.semaphore_wait(barrier, TP - 1 + 4)
    a_copies = spread(lambda peer: abuf.at[t], abuf.at[t], abuf, send_sem.at[0], recv_sem.at[0], "tp").start()
    both_ways(ring_sem.at[0], 2)
    pl.semaphore_wait(ring_sem.at[0], 2)
    both_ways(ring_sem.at[1], 4)
    a_copies.arrive()
    block = jnp.concatenate(
        [
            sum(abuf[k * per_tile + j].astype(F32) for j in range(per_tile))
            for k in range(TP // per_tile)
        ],
        axis=1,
    )
    ld_ng.wait()
    gain = jnp.concatenate([ng[k : k + 1, :] for k in range(width // LANES)], axis=1).astype(F32)
    scaled = (block * gain).astype(BF16)
    ld_wq.wait()
    ld_wk.wait()
    ld_wv.wait()
    proj = dot(scaled, wp[...])
    square = to_lanes(jnp.sum(block * block, axis=1, keepdims=True))
    key_at, value_at, last_at = heads * rows, (heads + 1) * rows, (heads + 2) * rows
    for g in range(heads + 2):
        psend[0, g * rows : (g + 1) * rows, :] = proj[:, g * LANES : (g + 1) * LANES].astype(BF16)
    psend[0, last_at:, :] = stacked(three(square)).astype(BF16)
    odd = lax.rem(z, 2)
    partner = lax.rem(KV + 1 - 2 * odd, KV)
    spread(
        lambda peer: psend.at[0], precv.at[0], precv, send_sem.at[0], recv_sem.at[9], "kv", [partner]
    ).start().arrive()
    pair = psend[0].astype(F32) + precv[0].astype(F32)
    square = pair[last_at : last_at + 1] + pair[last_at + 1 : last_at + 2]
    square = square + pair[last_at + 2 : last_at + 3]
    extra = stacked((square, square, *three(square)))
    at = iota((8, LANES), 0)
    queries = pair[0:key_at].astype(BF16)
    for j in range(KV):
        qsend[j, 0:key_at, :] = queries
        key_row = pair[key_at + j : key_at + j + 1]
        value_row = pair[value_at + j : value_at + j + 1]
        last = jnp.where(at == 0, key_row, jnp.where(at == 1, value_row, extra))
        qsend[j, key_at:, :] = last.astype(BF16)
    pairs = z // 2
    qbuf[pairs] = qsend[z]
    pl.semaphore_wait(ring_sem.at[1], 2)
    reach = [lax.rem(KV + (2 * odd - 1) * d, KV) for d in range(KV // 2 - 1, 0, -1)]
    q_copies = spread(
        lambda peer: qsend.at[peer], qbuf.at[pairs], qbuf, send_sem.at[0], recv_sem.at[1], "kv", reach
    ).start()
    ld_keys = load(keys_h, keys, 0)
    ld_values = load(values_h, values, 1)
    ld_lam = load(lam_h, lam, 2)
    ld_hg = load(hg_h, hg, 3)
    ld_wo = load(wo_h, wo, 4)
    ld_mg = load(mg_h, mg, 5)
    ld_wu = load(wu_h, wu, 6)
    ld_wd = load(wd_h, wd, 7)
    q_copies.arrive()
    q_sum = qbuf[0].astype(F32)
    for j in range(1, KV // 2):
        q_sum = q_sum + qbuf[j].astype(F32)
    r_sum = q_sum[heads * rows :]
    inv_lanes = lax.rsqrt((r_sum[2:3] + r_sum[3:4] + r_sum[4:5]) / D + EPS)
    inv_own = jnp.sum(
        jnp.where(iota(inv_lanes.shape, 1) == z, inv_lanes, 0.0), axis=1, keepdims=True
    )
    new_key = (inv_own * r_sum[0:1]).astype(BF16).astype(F32)
    new_value = (inv_own * r_sum[1:2]).astype(BF16).astype(F32)
    inv_rows = to_rows(inv_lanes, rows)

    lane = iota((rows, LANES), 1)
    for g in range(heads):
        head = (inv_rows * q_sum[g * rows : (g + 1) * rows]).astype(BF16)
        head = head.astype(F32) * (1.0 / half**0.5)
        for c in range(2):
            lined_s[pl.ds(2 * g + c, rows, stride=maps), :] = jnp.where(lane // half == c, head, 0.0)

    ld_keys.wait()
    ld_values.wait()
    seqs = 8 // maps
    group = iota((8, LANES), 0) // maps
    quarter = lines // 4
    mine = lax.rem(z, 4)
    for r in (0, 3, 1, 2):
        part_of = lax.rem(mine + r, 4)
        tops, totals, sums = [], [], []
        for u in range(quarter // 8):
            p = part_of * (quarter // 8) + u
            qp = lined_s[pl.ds(pl.multiple_of(8 * p, 8), 8), :]
            wide = jnp.concatenate([jnp.where(group == k, qp, 0.0) for k in range(seqs)], axis=1)
            wide_keys = jnp.concatenate([keys[seqs * p + k] for k in range(seqs)], axis=1)
            scores = lax.dot_general(
                wide.astype(BF16), wide_keys, (((1,), (1,)), ((), ())), preferred_element_type=F32
            )
            top = jnp.max(scores, axis=1, keepdims=True)
            expo = jnp.exp(scores - top)
            wide_values = jnp.concatenate([values[seqs * p + k] for k in range(seqs)], axis=1)
            part = dot(expo.astype(BF16), wide_values)
            weighted = part[:, 0:LANES]
            for k in range(1, seqs):
                weighted = jnp.where(group == k, part[:, k * LANES : (k + 1) * LANES], weighted)
            tops.append(top)
            totals.append(jnp.sum(expo, axis=1, keepdims=True))
            sums.append(weighted)
        top = jnp.concatenate(tops, axis=0)
        total = jnp.concatenate(totals, axis=0)
        weighted = jnp.concatenate(sums, axis=0)
        queries = lined_s[pl.ds(pl.multiple_of(quarter * part_of, quarter), quarter), :]
        own = jnp.sum(queries * new_key, axis=1, keepdims=True)
        sequence = part_of * (quarter // maps) + iota(own.shape, 0) // maps
        own = jnp.where(sequence == z, own, LOW)
        new_top = jnp.maximum(top, own)
        old_part = jnp.exp(top - new_top)
        own_part = jnp.exp(own - new_top)
        total = total * old_part + own_part
        weighted = weighted * old_part + own_part * new_value
        wsend[r, 0:quarter, :] = weighted.astype(BF16)
        both = stacked((*three(to_lanes(new_top)), *three(to_lanes(total))))
        wsend[r, quarter:, :] = both.astype(BF16)
        reach = sorted(range(r if r else 4, KV, 4), key=lambda d: -min(d, KV - d))
        spread(
            lambda peer: wsend.at[r], wbuf.at[z], wbuf, send_sem.at[0], recv_sem.at[2], "kv", reach
        ).start()
    wbuf[z] = wsend[0]
    w_copies = spread(lambda peer: wsend.at[0], wbuf.at[z], wbuf, send_sem.at[0], recv_sem.at[2], "kv")
    w_copies.arrive()
    tails = [wbuf[j, quarter:, :].astype(F32) for j in range(KV)]
    ml = jnp.concatenate([x[0:1] + x[1:2] + x[2:3] for x in tails], axis=0)
    totals = jnp.concatenate([x[3:4] + x[4:5] + x[5:6] for x in tails], axis=0)
    shares = jnp.exp(ml - jnp.max(ml, axis=0, keepdims=True))
    grand = jnp.sum(shares * totals, axis=0, keepdims=True)
    in_use = iota(ml.shape, 1) < quarter
    shares = jnp.where(in_use, shares / jnp.where(in_use[0:1], grand, 1.0), 0.0)
    columns = jnp.transpose(shares)
    attended = columns[0:quarter, 0:1] * wbuf[0, 0:quarter, :].astype(F32)
    for j in range(1, KV):
        attended = attended + columns[0:quarter, j : j + 1] * wbuf[j, 0:quarter, :].astype(F32)
    ld_lam.wait()
    ld_hg.wait()
    lambdas = lam[0:1, 0:1]
    for g in range(1, heads):
        lambdas = jnp.where(
            lax.rem(iota((quarter, 1), 0), maps) // 2 == g, lam[0:1, g : g + 1], lambdas
        )
    diff = attended - lambdas * pltpu.roll(attended, quarter - 1, 0)
    normed = (
        diff
        * lax.rsqrt(jnp.mean(diff * diff, axis=1, keepdims=True) + EPS)
        * hg[...].astype(F32)
    ).astype(BF16)
    nbuf[mine] = normed
    spread(lambda peer: nbuf.at[mine], nbuf.at[mine], nbuf, send_sem.at[0], recv_sem.at[3], "kv", (2, 1, KV - 1)).start().arrive()
    for c in range(4):
        lined_s[c * quarter : (c + 1) * quarter, :] = nbuf[c].astype(F32)
    outs = [lined_s[pl.ds(2 * g, rows, stride=maps), :] for g in range(heads)]
    heads_out = jnp.concatenate(outs, axis=1).astype(BF16)
    ld_wo.wait()
    dbuf[t] = dot(heads_out, wo[...]).astype(BF16)
    spread(lambda peer: dbuf.at[t], dbuf.at[t], dbuf, send_sem.at[0], recv_sem.at[4], "tp").start().arrive()
    projected = dbuf[0].astype(F32)
    for j in range(1, TP):
        projected = projected + dbuf[j].astype(F32)
    mixed = (block + projected).astype(BF16).astype(F32)
    sqbuf[z] = to_lanes(jnp.sum(mixed * mixed, axis=1, keepdims=True))
    ld_mg.wait()
    gain2 = jnp.concatenate([mg[k : k + 1, :] for k in range(width // LANES)], axis=1).astype(F32)
    scaled2 = (mixed * gain2).astype(BF16)
    ld_wu.wait()
    up = dot(scaled2, wu[...])
    owners = KV // 2
    owned = lax.rem(z, owners)
    share_width = up.shape[1] // owners
    for j in range(owners):
        us[j] = up[:, j * share_width : (j + 1) * share_width].astype(BF16)
    ur[z] = us[owned]
    u_copies = spread(lambda peer: us.at[lax.rem(peer, owners)], ur.at[z], ur, send_sem.at[0], recv_sem.at[5], "kv").start()
    u_copies.arrive()
    up_sum = ur[0].astype(F32)
    for j in range(1, KV):
        up_sum = up_sum + ur[j].astype(F32)
    act = jnp.maximum(up_sum, 0.0)
    hbuf[owned] = (act * act).astype(BF16)
    near = [owners // 2]
    for d in range(owners // 2 - 1, 0, -1):
        near += [d, KV - d]
    h_copies = spread(lambda peer: hbuf.at[owned], hbuf.at[owned], hbuf, send_sem.at[0], recv_sem.at[7], "kv", near).start()
    s_copies = spread(lambda peer: sqbuf.at[z], sqbuf.at[z], sqbuf, send_sem.at[1], recv_sem.at[6], "kv").start()
    h_copies.arrive()
    hidden = jnp.concatenate([hbuf[j] for j in range(owners)], axis=1)
    ld_wd.wait()
    down = dot(hidden, wd[...])
    for k in range(width // LANES):
        fs[k] = down[:, k * LANES : (k + 1) * LANES]
    fr[t] = fs[t // per_tile]
    f_copies = spread(lambda peer: fs.at[peer // per_tile], fr.at[t], fr, send_sem.at[0], recv_sem.at[8], "tp").start()
    s_copies.arrive()
    square2 = sqbuf[0]
    for j in range(1, KV):
        square2 = square2 + sqbuf[j]
    inv2 = to_rows(1.0 / (square2 / D + EPS), rows)
    f_copies.arrive()
    y = fr[0]
    for j in range(1, TP):
        y = y + fr[j]
    y = inv2 * y
    for k in range(width // LANES):
        y = y + jnp.where(t // per_tile == k, mixed[:, k * LANES : (k + 1) * LANES], 0.0)
    result = y[:, 0:piece]
    for k in range(1, per_tile):
        result = jnp.where(lax.rem(t, per_tile) == k, y[:, k * piece : (k + 1) * piece], result)
    out_ref[...] = result.astype(out_ref.dtype)


def body(
    KV,
    TP,
    residual,
    cache_keys,
    cache_values,
    norm_gain,
    query_weight,
    key_weight,
    value_weight,
    head_lambda,
    head_gain,
    out_weight,
    mixer_gain,
    up_weight,
    down_weight,
):
    rows, piece = residual.shape
    positions, depth = cache_keys.shape[1], cache_keys.shape[3]
    width = out_weight.shape[1]
    qcols = query_weight.shape[1]
    lines = rows * qcols * 2 // LANES
    share = up_weight.shape[1] * 2 // KV
    any_spec = pl.BlockSpec(memory_space=pl.ANY)
    dma = pltpu.SemaphoreType.DMA
    keys = cache_keys.reshape(rows, positions, depth)
    values = cache_values.reshape(rows, positions, depth)
    args = (
        residual,
        keys,
        values,
        norm_gain.reshape(width // LANES, LANES),
        query_weight,
        key_weight,
        value_weight,
        head_lambda.reshape(1, -1),
        head_gain.reshape(1, -1),
        out_weight,
        mixer_gain.reshape(width // LANES, LANES),
        up_weight,
        down_weight,
    )
    return pl.pallas_call(
        functools.partial(kernel, KV, TP),
        out_shape=jax.ShapeDtypeStruct((rows, piece), residual.dtype),
        in_specs=[any_spec] * len(args),
        out_specs=pl.BlockSpec(memory_space=pltpu.VMEM),
        scratch_shapes=[
            pltpu.VMEM((rows, piece), BF16),
            pltpu.VMEM(keys.shape, BF16),
            pltpu.VMEM(values.shape, BF16),
            pltpu.VMEM((width // LANES, LANES), BF16),
            pltpu.VMEM((width, qcols + 2 * LANES), BF16),
            pltpu.VMEM((1, head_lambda.shape[0]), F32),
            pltpu.VMEM((1, head_gain.shape[0]), BF16),
            pltpu.VMEM(out_weight.shape, BF16),
            pltpu.VMEM((width // LANES, LANES), BF16),
            pltpu.VMEM(up_weight.shape, BF16),
            pltpu.VMEM(down_weight.shape, BF16),
            pltpu.VMEM((TP, rows, LANES), BF16),
            *[pltpu.VMEM((1, rows * (qcols // LANES + 2) + 8, LANES), BF16)] * 2,
            pltpu.VMEM((KV, rows * qcols // LANES + 8, LANES), BF16),
            pltpu.VMEM((KV // 2, rows * qcols // LANES + 8, LANES), BF16),
            pltpu.VMEM((lines, LANES), F32),
            pltpu.VMEM((4, lines // 4 + 8, LANES), BF16),
            pltpu.VMEM((KV, lines // 4 + 8, LANES), BF16),
            pltpu.VMEM((4, lines // 4, LANES), BF16),
            pltpu.VMEM((TP, rows, width), BF16),
            pltpu.VMEM((KV, 1, LANES), F32),
            pltpu.VMEM((KV // 2, rows, share), BF16),
            pltpu.VMEM((KV, rows, share), BF16),
            pltpu.VMEM((KV // 2, rows, share), BF16),
            pltpu.VMEM((width // LANES, rows, LANES), F32),
            pltpu.VMEM((TP, rows, LANES), F32),
            pltpu.SemaphoreType.REGULAR((2,)),
            dma((8,)),
            dma((2,)),
            dma((10,)),
        ],
        compiler_params=pltpu.CompilerParams(
            collective_id=0, has_side_effects=True, vmem_limit_bytes=64 * 1000 * 1000
        ),
        name="layer",
    )(*args)


def solution(mesh):
    in_specs = (
        P("grp", ("kv", "tp")),
        P("grp", "kv", "tp", None),
        P("grp", "kv", "tp", None),
        P("kv"),
        P("kv", "tp"),
        P("kv", "tp"),
        P("kv", "tp"),
        P("tp"),
        P(),
        P("tp", "kv"),
        P("kv"),
        P("kv", "tp"),
        P("tp", "kv"),
    )
    out_specs = P("grp", ("kv", "tp"))
    fn = functools.partial(body, mesh.shape["kv"], mesh.shape["tp"])
    return jax.shard_map(fn, mesh=mesh, in_specs=in_specs, out_specs=out_specs, check_vma=False)
```
